32 devices in a mesh: sp: 8 (over z, x), tp: 4 (over y, core).
Axes of the slice: x: 2, y: 2, z: 4, core: 2. Of those that a mesh axis runs over, the one named last changes fastest.
Arguments:
- residual_in: bfloat16 [1536, 2048], P('sp', 'tp'), may hold values from -6 to 6
- query_rows: bfloat16 [1536, 1024], P('sp', 'tp'), may hold values from -8 to 8
- key_rows: bfloat16 [1536, 1024], P('sp', 'tp'), may hold values from -8 to 8
- value_rows: bfloat16 [1536, 1024], P('sp', 'tp'), may hold values from -6 to 6
- map_weight: float32 [16], P('tp'), may hold values from 0.3 to 0.8
- head_gain: float32 [64], replicated, may hold values from 0.1 to 1.9
- out_proj: bfloat16 [1024, 2048], P(None, 'tp'), may hold values from -0.1875 to 0.1875
- norm_gain: float32 [2048], replicated, may hold values from 0.1 to 1.9
- route_ids: int32 [1536, 2], P('sp'), may hold values from 0 to 7, all different within a row; in each aligned block of 192 rows (0 to 191, 192 to 383, ...) at most 60 rows name the same one
- route_weights: float32 [1536, 2], P('sp'), may hold values from 0.2 to 1.2
- expert_gate: bfloat16 [8, 1024, 2048], P('sp', 'tp'), may hold values from -0.125 to 0.125
- expert_up: bfloat16 [8, 1024, 2048], P('sp', 'tp'), may hold values from -0.125 to 0.125
- expert_down: bfloat16 [8, 1024, 2048], P('sp', None, 'tp'), may hold values from -0.1875 to 0.1875
- shared_gate: bfloat16 [1024, 2048], P('tp'), may hold values from -0.125 to 0.125
- shared_up: bfloat16 [1024, 2048], P('tp'), may hold values from -0.125 to 0.125
- shared_down: bfloat16 [1024, 2048], P(None, 'tp'), may hold values from -0.1875 to 0.1875
Outputs:
- mixed_out: bfloat16 [1536, 2048], P('sp', 'tp')
The draws below stay inside these ranges and needn't reach their ends.
Inputs may be any that keep to these rules, and one draw needn't show every extreme that they name: `route_ids`: each row names 2 different experts. Among the rows held by one index of sp no expert is named more than 60 times, and in every draw some expert is named exactly 60 times by the rows of some index of sp.
All inputs are finite; a program needn't handle non-finite values.
Results may differ from the reference program's by a relative error of at most 0.0095.
Values may be sent and summed in bfloat16 or wider, within the bound.
A program may use at most 64 MiB of HBM per device.

```python
import math
from functools import partial
import jax
import jax.numpy as jnp
import numpy as np
from jax import lax

D = 2048
H = 16
HD = 64
FE = 1024
TOPK = 2
SEQ_DEV = 192
TOKENS = 1536
EXPERTS = 8
CAPACITY = 60
N_SP = 8


def query_key_pair(key):
    query_key = jax.random.fold_in(key, 11)
    second_key = jax.random.fold_in(key, 12)
    full_shape = (TOKENS, H * HD)
    queries = jnp.clip(jax.random.normal(query_key, full_shape, jnp.float32) * 1.3, -8.0, 8.0)
    key_vals = jnp.clip(jax.random.normal(second_key, full_shape, jnp.float32) * 1.3, -8.0, 8.0)
    return (queries, key_vals)


def draw_query_rows(key, part):
    return query_key_pair(key)[0].astype(jnp.bfloat16)


def draw_key_rows(key, part):
    return query_key_pair(key)[1].astype(jnp.bfloat16)


def block_scale(rng, extent, pieces, low, high):
    def one(dim, shards_of):
        heights = jax.random.uniform(jax.random.fold_in(jax.random.fold_in(rng, 6), dim), (shards_of,), jnp.float32, low / len(pieces), high / len(pieces))
        return jnp.repeat(jnp.exp(heights), extent[dim] // shards_of).reshape((-1,) + (1,) * (len(extent) - dim - 1))

    loudness = one(*pieces[0])
    for cut in pieces[1:]:
        loudness = loudness * one(*cut)
    return loudness


def deal_out(rng, own, number, rows, number_of, top, reach, slope):
    ranking = jax.random.permutation(rng, number_of)
    packed, usual = shares(number_of, rows * top, reach, slope, True), shares(number_of, rows * top, reach, slope, False)
    places = jnp.arange(number_of)

    def named(lengths, rotation):
        used = int((lengths > 0).sum())
        fixed = max(1, used // 4)
        passed = fixed + (places - fixed + rotation * (used - fixed)) % max(1, number_of - fixed)
        return jnp.zeros((number_of,), jnp.int32).at[ranking[jnp.where(places < fixed, places, passed)]].set(jnp.asarray(lengths, jnp.int32))

    lengths = jnp.where(number % 4 == 0, named(packed, number // 4), named(usual, number - number // 4 - 1))
    mixed = jax.random.permutation(jax.random.fold_in(own, 3), number_of)
    donor, receiver = mixed[0:number_of // 2 * 2:2], mixed[1:number_of // 2 * 2:2]
    slack = jnp.minimum(lengths[donor] - 1, reach - lengths[receiver]) // 2
    slack = jnp.where((donor == ranking[0]) | (receiver == ranking[0]) | (lengths[receiver] == 0), 0, jnp.maximum(slack, 0))
    passed = jax.random.randint(jax.random.fold_in(own, 4), (number_of // 2,), 0, 1 << 20) % (slack + 1)
    lengths = lengths.at[donor].add(-passed).at[receiver].add(passed)
    items = jnp.searchsorted(jnp.cumsum(lengths), jnp.arange(rows * top), side="right").astype(jnp.int32)
    listing = items.reshape(top, rows).T
    listing = listing[jax.random.permutation(jax.random.fold_in(own, 1), rows)]
    rotation = jax.random.randint(jax.random.fold_in(own, 2), (rows, 1), 0, top)
    return jnp.take_along_axis(listing, (jnp.arange(top)[None, :] + rotation) % top, axis=1)


def shares(amount, total, most, skew, full):
    loads = [(1 << 20) // math.isqrt(grade ** skew) + 1 for grade in range(1, amount + 1)]
    largest = most if full else min(most, max(-(-total // amount), total * loads[0] // sum(loads)))
    least = 1 if total - largest >= amount - 1 else 0
    given, rest = [largest] + [least] * (amount - 1), total - largest - least * (amount - 1)
    while rest > 0:
        movable = [i for i in range(1, amount) if given[i] < largest] or [i for i in range(1, amount) if given[i] < most]
        mass, remaining = sum([loads[i] for i in movable]), rest
        for i in movable:
            extra = min(most - given[i], max(1, remaining * loads[i] // mass), rest)
            given[i] = given[i] + extra
            rest = rest - extra
    return np.array(given)


def gaussian(rng, extent, spread, reach, cuts=(), kind=jnp.bfloat16):
    entries = spread * jax.random.normal(rng, extent, jnp.float32)
    if cuts:
        entries = entries * block_scale(rng, extent, cuts, -0.22, 0.18)
    return jnp.clip(entries, -reach, reach).astype(kind)


def setup_inputs(seed: int = 0) -> dict:
    seeds = jax.random.split(jax.random.key(seed), 17)
    residual_in = gaussian(seeds[0], (TOKENS, D), 1.0, 6.0, ((0, 8), (1, 4)))
    query_rows = draw_query_rows(jax.random.fold_in(seeds[16], 71), 0)
    key_rows = draw_key_rows(jax.random.fold_in(seeds[16], 71), 0)
    value_rows = gaussian(seeds[3], (TOKENS, H * HD), 1.0, 6.0, ((0, 8), (1, 4)))
    map_weight = jnp.clip(0.3 + 0.5 * jax.random.uniform(seeds[4], (H,), jnp.float32) ** block_scale(seeds[4], (H,), ((0, 4),), -0.2, 0.2), 0.3, 0.8)
    head_gain = jnp.clip(1.0 + 0.18 * jax.random.normal(seeds[5], (HD,), jnp.float32), 0.1, 1.9)
    out_proj = gaussian(seeds[6], (H * HD, D), (H * HD) ** -0.5, 0.1875, ((1, 4),))
    norm_gain = jnp.clip(1.0 + 0.18 * jax.random.normal(seeds[7], (D,), jnp.float32), 0.1, 1.9)
    route_ids_keys = jax.random.split(jax.random.fold_in(seeds[8], 1), TOKENS // SEQ_DEV)
    route_ids_turns = jax.random.permutation(jax.random.fold_in(seeds[8], 3), TOKENS // SEQ_DEV)
    route_ids = jax.vmap(lambda own, number: deal_out(jax.random.fold_in(seeds[8], 2), own, number, SEQ_DEV, EXPERTS, TOPK, CAPACITY, 2))(route_ids_keys, route_ids_turns).reshape((TOKENS, TOPK))
    route_weights = jnp.clip(0.2 + 1 * jax.random.uniform(seeds[9], (TOKENS, TOPK), jnp.float32) ** block_scale(seeds[9], (TOKENS, TOPK), ((0, 8),), -0.2, 0.2), 0.2, 1.2)
    expert_gate = gaussian(seeds[10], (EXPERTS, FE, D), D ** -0.5, 0.125, ((0, 8), (1, 4)))
    expert_up = gaussian(seeds[11], (EXPERTS, FE, D), D ** -0.5, 0.125, ((0, 8), (1, 4)))
    expert_down = gaussian(seeds[12], (EXPERTS, FE, D), FE ** -0.5, 0.1875, ((0, 8), (2, 4)))
    shared_gate = gaussian(seeds[13], (FE, D), D ** -0.5, 0.125, ((0, 4),))
    shared_up = gaussian(seeds[14], (FE, D), D ** -0.5, 0.125, ((0, 4),))
    shared_down = gaussian(seeds[15], (FE, D), FE ** -0.5, 0.1875, ((1, 4),))
    return {"residual_in": residual_in, "query_rows": query_rows, "key_rows": key_rows, "value_rows": value_rows, "map_weight": map_weight, "head_gain": head_gain, "out_proj": out_proj, "norm_gain": norm_gain, "route_ids": route_ids, "route_weights": route_weights, "expert_gate": expert_gate, "expert_up": expert_up, "expert_down": expert_down, "shared_gate": shared_gate, "shared_up": shared_up, "shared_down": shared_down}


epsilon = 1e-06
masked_score = -1e+30

def rms_scale(values, gain_vec):
    squares = lax.optimization_barrier(jnp.mean(values * values, axis=-1, keepdims=True))
    return values * lax.rsqrt(squares + epsilon) * gain_vec

def block_slots(route_block, experts_all, capacity):
    flat_ids = route_block.reshape(-1)
    one_hot = (flat_ids[:, None] == jnp.arange(experts_all, dtype=jnp.int32)[None, :]).astype(jnp.int32)
    earlier = jnp.cumsum(one_hot, axis=0) - one_hot
    position = lax.optimization_barrier(jnp.sum(earlier * one_hot, axis=1))
    return (flat_ids * capacity + position).astype(jnp.int32).reshape(route_block.shape)

def reference(residual_in, query_rows, key_rows, value_rows, map_weight, head_gain, out_proj, norm_gain, route_ids, route_weights, expert_gate, expert_up, expert_down, shared_gate, shared_up, shared_down):
    half_dim = HD // 2
    block_len = min(256, TOKENS)
    block_count = TOKENS // block_len
    key_heads = key_rows.reshape(TOKENS, H, 2, half_dim).astype(jnp.float32)
    value_heads = value_rows.reshape(TOKENS, H, HD).astype(jnp.float32)
    query_blocks = query_rows.reshape(block_count, block_len, H, 2, half_dim)
    key_pos = jnp.arange(TOKENS, dtype=jnp.int32)

    def attend(operands):
        query_block, block_index = operands
        query_pos = block_index * block_len + jnp.arange(block_len, dtype=jnp.int32)
        scores = jnp.einsum('qhmd,khmd->mhqk', query_block.astype(jnp.float32), key_heads) * half_dim ** (-0.5)
        visible = key_pos[None, :] <= query_pos[:, None]
        scores = jnp.where(visible, scores, masked_score)
        row_max = lax.optimization_barrier(jnp.max(scores, axis=-1, keepdims=True))
        expo = jnp.where(visible, jnp.exp(scores - row_max), 0.0)
        totals = lax.optimization_barrier(jnp.sum(expo, axis=-1))
        rounded = lax.optimization_barrier(expo.astype(jnp.bfloat16)).astype(jnp.float32)
        summed = jnp.einsum('mhqk,khd->mhqd', rounded, value_heads) / totals[..., None]
        return summed[0] - map_weight[:, None, None] * summed[1]
    parts = lax.map(attend, (query_blocks, jnp.arange(block_count, dtype=jnp.int32)))
    head_out = rms_scale(parts, head_gain).astype(jnp.bfloat16)
    head_out = jnp.transpose(head_out, (0, 2, 1, 3)).reshape(TOKENS, H * HD)
    attn = jnp.dot(head_out, out_proj, preferred_element_type=jnp.float32)
    hidden_state = (residual_in.astype(jnp.float32) + attn).astype(jnp.bfloat16)
    normed = rms_scale(hidden_state.astype(jnp.float32), norm_gain).astype(jnp.bfloat16)
    shared_hidden = (jax.nn.silu(jnp.dot(normed, shared_gate.T, preferred_element_type=jnp.float32)) * jnp.dot(normed, shared_up.T, preferred_element_type=jnp.float32)).astype(jnp.bfloat16)
    shared_out = jnp.dot(shared_hidden, shared_down, preferred_element_type=jnp.float32)
    slot_ids = jax.vmap(partial(block_slots, experts_all=EXPERTS, capacity=CAPACITY))(route_ids.reshape(N_SP, SEQ_DEV, TOPK))
    group_ids = jnp.broadcast_to(jnp.arange(N_SP, dtype=jnp.int32)[:, None, None], slot_ids.shape)
    token_ids = group_ids * SEQ_DEV + jnp.broadcast_to(jnp.arange(SEQ_DEV, dtype=jnp.int32)[None, :, None], slot_ids.shape)
    table = jnp.full((N_SP, EXPERTS * CAPACITY), TOKENS, jnp.int32).at[group_ids, slot_ids].set(token_ids)
    table = jnp.transpose(table.reshape(N_SP, EXPERTS, CAPACITY), (1, 0, 2))
    padded = jnp.concatenate([normed, jnp.zeros((1, D), jnp.bfloat16)], axis=0)

    def run_expert(operands):
        gate_w, up_w, down_w, rows_index = operands
        gathered = padded[rows_index.reshape(-1)]
        hidden_part = (jax.nn.silu(jnp.dot(gathered, gate_w.T, preferred_element_type=jnp.float32)) * jnp.dot(gathered, up_w.T, preferred_element_type=jnp.float32)).astype(jnp.bfloat16)
        return jnp.dot(hidden_part, down_w, preferred_element_type=jnp.float32).astype(jnp.bfloat16)
    results = lax.map(run_expert, (expert_gate, expert_up, expert_down, table))
    results = results.reshape(EXPERTS * N_SP * CAPACITY, D)
    expert_of = slot_ids // CAPACITY
    position = slot_ids % CAPACITY
    flat_index = ((expert_of * N_SP + group_ids) * CAPACITY + position).astype(jnp.int32).reshape(TOKENS, TOPK)
    picked = results[flat_index].astype(jnp.float32)
    routed = lax.optimization_barrier(jnp.sum(picked * route_weights[:, :, None], axis=1))
    return (hidden_state.astype(jnp.float32) + shared_out + routed).astype(jnp.bfloat16)
```

```python
import functools

import jax
import jax.numpy as jnp
from jax import lax
from jax.experimental import pallas as pl
from jax.experimental.pallas import tpu as pltpu
from jax.sharding import PartitionSpec as P

epsilon = 1e-06
masked_score = -1e30
MESH = pl.DeviceIdType.MESH


def rms_scale(values, gain_vec):
    squares = jnp.mean(values * values, axis=-1, keepdims=True)
    return values * lax.rsqrt(squares + epsilon) * gain_vec


def block_slots(route_block, experts_all, capacity):
    flat_ids = route_block.reshape(-1)
    one_hot = (flat_ids[:, None] == jnp.arange(experts_all, dtype=jnp.int32)[None, :]).astype(
        jnp.int32
    )
    earlier = jnp.cumsum(one_hot, axis=0) - one_hot
    position = jnp.sum(earlier * one_hot, axis=1)
    return (flat_ids * capacity + position).reshape(route_block.shape)


def body(
    residual_in,
    query_rows,
    key_rows,
    value_rows,
    map_weight,
    head_gain,
    out_proj,
    norm_gain,
    route_ids,
    route_weights,
    expert_gate,
    expert_up,
    expert_down,
    shared_gate,
    shared_up,
    shared_down,
):
    seq_dev = residual_in.shape[0]
    col_dev = residual_in.shape[1]
    heads_here = map_weight.shape[0]
    head_dim = head_gain.shape[0]
    half_dim = head_dim // 2
    topk_count = route_ids.shape[1]
    exp_here = expert_gate.shape[0]
    experts_all = exp_here * lax.axis_size("sp")
    capacity = 5 * seq_dev * topk_count // (4 * experts_all)
    score_scale = half_dim ** (-0.5)
    query_pos = lax.axis_index("sp") * seq_dev + jnp.arange(seq_dev, dtype=jnp.int32)
    query_heads = query_rows.reshape(seq_dev, heads_here, 2, half_dim)
    key_piece = lax.all_gather(key_rows, "sp", axis=0, tiled=True)
    value_piece = lax.all_gather(value_rows, "sp", axis=0, tiled=True)
    piece_len = key_piece.shape[0]
    key_heads = key_piece.reshape(piece_len, heads_here, 2, half_dim)
    value_heads = value_piece.reshape(piece_len, heads_here, head_dim)
    scores = (
        jnp.einsum("qhmd,khmd->mhqk", query_heads, key_heads, preferred_element_type=jnp.float32)
        * score_scale
    )
    key_pos = jnp.arange(piece_len, dtype=jnp.int32)
    visible = key_pos[None, :] <= query_pos[:, None]
    scores = jnp.where(visible, scores, masked_score)
    run_max = jnp.full((2, heads_here, seq_dev), masked_score, jnp.float32)
    new_max = jnp.maximum(run_max, jnp.max(scores, axis=-1))
    expo = jnp.where(visible, jnp.exp(scores - new_max[..., None]), 0.0)
    new_sum = jnp.sum(expo, axis=-1)
    product = jnp.einsum(
        "mhqk,khd->mhqd", expo.astype(jnp.bfloat16), value_heads, preferred_element_type=jnp.float32
    )
    summed = product / new_sum[..., None]
    diff_out = summed[0] - map_weight[:, None, None] * summed[1]
    head_out = rms_scale(diff_out, head_gain).astype(jnp.bfloat16)
    head_out = jnp.transpose(head_out, (1, 0, 2)).reshape(seq_dev, heads_here * head_dim)
    attn = jnp.dot(
        lax.all_gather(head_out, "tp", axis=1, tiled=True),
        out_proj,
        preferred_element_type=jnp.float32,
    )
    hidden_state = (residual_in.astype(jnp.float32) + attn).astype(jnp.bfloat16)
    full_rows = lax.all_gather(hidden_state, "tp", axis=1, tiled=True)
    normed = rms_scale(full_rows.astype(jnp.float32), norm_gain).astype(jnp.bfloat16)
    shared_gate_part = jnp.einsum(
        "rd,fd->rf", normed, shared_gate, preferred_element_type=jnp.float32
    )
    shared_up_part = jnp.einsum("rd,fd->rf", normed, shared_up, preferred_element_type=jnp.float32)
    shared_hidden = (jax.nn.silu(shared_gate_part) * shared_up_part).astype(jnp.bfloat16)
    slot_ids = block_slots(route_ids, experts_all, capacity)
    token_of = jnp.repeat(jnp.arange(seq_dev, dtype=jnp.int32), topk_count)
    slot_token = (
        jnp.full((experts_all * capacity,), seq_dev, jnp.int32)
        .at[slot_ids.reshape(-1)]
        .set(token_of)
    )
    own_cols = lax.dynamic_slice_in_dim(normed, lax.axis_index("tp") * col_dev, col_dev, 1)
    padded = jnp.concatenate([own_cols, jnp.zeros((1, col_dev), jnp.bfloat16)], axis=0)
    outgoing = jnp.take(padded, slot_token, axis=0).reshape(experts_all, capacity, col_dev)
    arrived = lax.all_to_all(outgoing, "sp", split_axis=0, concat_axis=1, tiled=True)
    arrived_rows = arrived.shape[1]
    pieces = lax.all_gather(arrived, "tp", axis=2, tiled=True)
    gate_add = jnp.einsum("erd,efd->erf", pieces, expert_gate, preferred_element_type=jnp.float32)
    up_add = jnp.einsum("erd,efd->erf", pieces, expert_up, preferred_element_type=jnp.float32)
    expert_hidden = (jax.nn.silu(gate_add) * up_add).astype(jnp.bfloat16)
    expert_flat = expert_hidden.reshape(exp_here * arrived_rows, expert_hidden.shape[2])
    pieces = (
        lax.all_gather(shared_hidden, "tp", axis=1, tiled=True),
        lax.all_gather(expert_flat, "tp", axis=1, tiled=True),
    )
    piece_width = pieces[0].shape[1]
    routed_piece = pieces[1].reshape(exp_here, arrived_rows, piece_width)
    shared_add = jnp.dot(pieces[0], shared_down, preferred_element_type=jnp.float32)
    expert_add = jnp.einsum(
        "erf,efd->erd", routed_piece, expert_down, preferred_element_type=jnp.float32
    )
    returned_rows = lax.all_to_all(
        expert_add.astype(jnp.bfloat16), "sp", split_axis=1, concat_axis=0, tiled=True
    )
    returned_flat = returned_rows.reshape(experts_all * capacity, col_dev)
    picked = (
        jnp.take(returned_flat, slot_ids.reshape(-1), axis=0)
        .reshape(seq_dev, topk_count, col_dev)
        .astype(jnp.float32)
    )
    routed = jnp.sum(picked * route_weights[:, :, None], axis=1)
    return (hidden_state.astype(jnp.float32) + shared_add + routed).astype(jnp.bfloat16)


def lane_iota(rows):
    return lax.broadcasted_iota(jnp.int32, (rows, 128), 1)


def roll_half(values):
    return pltpu.roll(values, 64, 1)


def contract_last(a, b):
    return lax.dot_general(a, b, (((1,), (1,)), ((), ())), preferred_element_type=jnp.float32)


def layer_kernel(
    n_sp,
    n_tp,
    q_in,
    k_in,
    v_in,
    res_in,
    map_w,
    head_g,
    norm_g,
    slot_row,
    slot_col,
    route_w,
    out_proj,
    exp_gate,
    exp_up,
    exp_down,
    sh_gate,
    sh_up,
    sh_down,
    out_ref,
    w_out,
    w_gate,
    w_up,
    w_down,
    w_sgate,
    w_sup,
    w_sdown,
    kv_out,
    q_out,
    kv_buf,
    q_buf,
    o_out,
    ho_buf,
    hid_buf,
    disp_out,
    arr_buf,
    sh_buf,
    eh_buf,
    res_out,
    ret_buf,
    w_sem,
    a_send,
    kv_recv,
    q_recv,
    o_send,
    o_recv,
    d_send,
    d_recv,
    r_send,
    r_recv,
    g_send,
    g_recv,
):
    me_s = lax.axis_index("sp")
    me_t = lax.axis_index("tp")
    sib = me_t + 1 - 2 * lax.rem(me_t, 2)
    peers = n_tp // 2 - 1
    rows = res_in.shape[0]
    col_dev = res_in.shape[1]
    half = rows // 2
    quarter = rows // 4
    cap = arr_buf.shape[2]
    half_dim = 32
    groups = eh_buf.shape[1]
    per_group = n_sp // groups
    bf16 = jnp.bfloat16
    f32 = jnp.float32

    loads = []
    for i, (src, dst) in enumerate(
        (
            (out_proj, w_out),
            (sh_gate, w_sgate),
            (sh_up, w_sup),
            (exp_gate.at[0], w_gate),
            (exp_up.at[0], w_up),
            (exp_down.at[0], w_down),
            (sh_down, w_sdown),
        )
    ):
        copy = pltpu.make_async_copy(src, dst, w_sem.at[i])
        copy.start()
        loads.append(copy)

    barrier = pltpu.get_barrier_semaphore()
    for d in range(1, n_sp):
        pl.semaphore_signal(
            barrier, inc=1, device_id={"sp": lax.rem(me_s + d, n_sp)}, device_id_type=MESH
        )
    for d in range(1, n_tp):
        pl.semaphore_signal(
            barrier, inc=1, device_id={"tp": lax.rem(me_t + d, n_tp)}, device_id_type=MESH
        )

    sends = []

    def send(src, dst, ssem, rsem, device):
        copy = pltpu.make_async_remote_copy(
            src_ref=src,
            dst_ref=dst,
            send_sem=ssem,
            recv_sem=rsem,
            device_id=device,
            device_id_type=MESH,
        )
        copy.start()
        return copy

    def wait_recv(ref, ssem, rsem, device):
        pltpu.make_async_remote_copy(
            src_ref=ref,
            dst_ref=ref,
            send_sem=ssem,
            recv_sem=rsem,
            device_id=device,
            device_id_type=MESH,
        ).wait_recv()

    n_gs = 1 + 2 * peers

    def gather_start(piece, get):
        for k in range(1, peers + 1):
            other = lax.rem(me_t + 2 * k, n_tp)
            sends.append(
                send(
                    get(me_t),
                    get(me_t),
                    g_send.at[piece * n_gs + k],
                    g_recv.at[piece * n_tp + me_t],
                    {"tp": other},
                )
            )
        sends.append(
            send(
                get(me_t),
                get(me_t),
                g_send.at[piece * n_gs],
                g_recv.at[piece * n_tp + me_t],
                {"tp": sib},
            )
        )

    def gather_relay(piece, get):
        for k in range(1, peers + 1):
            other = lax.rem(me_t + 2 * k, n_tp)
            wait_recv(
                get(other), g_send.at[piece * n_gs], g_recv.at[piece * n_tp + other], {"tp": sib}
            )
            sends.append(
                send(
                    get(other),
                    get(other),
                    g_send.at[piece * n_gs + peers + k],
                    g_recv.at[piece * n_tp + other],
                    {"tp": sib},
                )
            )

    def gather_finish(piece, get):
        for k in range(peers + 1):
            other = lax.rem(sib + 2 * k, n_tp)
            wait_recv(
                get(other), g_send.at[piece * n_gs], g_recv.at[piece * n_tp + other], {"tp": sib}
            )

    low_rows = lane_iota(rows) < 64
    low_quarter = lane_iota(quarter) < 64
    for j in range(n_sp // 4):
        pair = slice(j * 128, (j + 1) * 128)
        keys = k_in[:, pair].astype(f32)
        vals = v_in[:, pair].astype(f32)
        kv_out[2 * j] = jnp.where(low_rows, keys, roll_half(vals)).astype(bf16)
        kv_out[2 * j + 1] = jnp.where(low_rows, roll_half(keys), vals).astype(bf16)
        for p in range(2):
            first = q_in[p * half : p * half + quarter, pair].astype(f32)
            second = q_in[p * half + quarter : (p + 1) * half, pair].astype(f32)
            q_out[4 * j + p] = jnp.where(low_quarter, first, roll_half(second)).astype(bf16)
            q_out[4 * j + 2 + p] = jnp.where(low_quarter, roll_half(first), second).astype(bf16)

    pl.semaphore_wait(barrier, n_sp + n_tp - 2)

    for d in range(1, n_sp):
        dst = lax.rem(me_s + d, n_sp)
        sends.append(
            send(
                kv_out.at[dst // 2],
                kv_buf.at[me_s],
                a_send.at[2 * d],
                kv_recv.at[me_s],
                {"sp": dst},
            )
        )
        sends.append(
            send(
                q_out.at[dst], q_buf.at[me_s], a_send.at[2 * d + 1], q_recv.at[me_s], {"sp": dst}
            )
        )
    kv_buf[me_s] = kv_out[me_s // 2]
    q_buf[me_s] = q_out[me_s]

    parity = lax.rem(me_s, 2)
    lane_q = lane_iota(quarter)
    scale = half_dim ** (-0.5)
    row_in = lax.broadcasted_iota(jnp.int32, (half, rows), 0) + parity * half
    visible_half = lax.broadcasted_iota(jnp.int32, (half, rows), 1) <= row_in
    visible = jnp.concatenate([visible_half.astype(f32)] * 2, axis=0) > 0.5
    high_lanes = lane_iota(half) >= 64
    zero_q = jnp.zeros((quarter, 128), f32)
    for s in range(n_sp):

        @pl.when(me_s != s)
        def _():
            wait_recv(kv_buf.at[s], a_send.at[0], kv_recv.at[s], {"sp": s})
            wait_recv(q_buf.at[s], a_send.at[1], q_recv.at[s], {"sp": s})

        packed = q_buf[s].astype(f32)
        rolled = roll_half(packed)
        first_map = lane_q < 32
        second_map = (lane_q >= 32) & (lane_q < 64)
        queries = jnp.concatenate(
            [
                jnp.where(first_map, packed, zero_q),
                jnp.where(first_map, rolled, zero_q),
                jnp.where(second_map, packed, zero_q),
                jnp.where(second_map, rolled, zero_q),
            ],
            axis=0,
        ).astype(bf16)
        diag = contract_last(queries, kv_buf[s]) * scale
        diag = jnp.where(visible, diag, masked_score)
        row_max = jnp.max(diag, axis=1, keepdims=True)
        if s:
            before = kv_buf[0:s].reshape(s * rows, 128)
            early = contract_last(queries, before) * scale
            row_max = jnp.maximum(row_max, jnp.max(early, axis=1, keepdims=True))
        expo = jnp.where(visible, jnp.exp(diag - row_max), 0.0)
        total = jnp.sum(expo, axis=1, keepdims=True)
        acc = jnp.dot(expo.astype(bf16), kv_buf[s], preferred_element_type=f32)
        if s:
            expo_early = jnp.exp(early - row_max)
            total = total + jnp.sum(expo_early, axis=1, keepdims=True)
            acc = acc + jnp.dot(expo_early.astype(bf16), before, preferred_element_type=f32)
        summed = acc / total
        diff = summed[0:half] - map_w[...] * summed[half:rows]
        diff = jnp.where(high_lanes, diff, 0.0)
        squares = jnp.sum(diff * diff, axis=1, keepdims=True) * (1.0 / 64.0)
        head = diff * lax.rsqrt(squares + epsilon) * head_g[...]
        o_out[s] = (roll_half(head[0:quarter]) + head[quarter:half]).astype(bf16)

        @pl.when(me_s != s)
        def _():
            send(
                o_out.at[s],
                ho_buf.at[me_t, me_s],
                o_send.at[s],
                o_recv.at[me_s],
                {"sp": s},
            )

        @pl.when(me_s == s)
        def _():
            ho_buf[me_t, s] = o_out[s]

    for s in range(n_sp):

        @pl.when(me_s != s)
        def _():
            wait_recv(ho_buf.at[me_t, s], o_send.at[s], o_recv.at[s], {"sp": s})

    def get_ho(t):
        return ho_buf.at[t]

    gather_start(0, get_ho)

    slots = n_sp * cap
    slot_iota = lax.broadcasted_iota(jnp.int32, (slots, rows), 0)
    chosen = (slot_iota == slot_row[0:1, :]) | (slot_iota == slot_row[1:2, :])
    spread = jnp.where(chosen, 1.0, 0.0).astype(bf16)
    gather_relay(0, get_ho)
    gather_finish(0, get_ho)

    blocks = []
    for p in range(2):
        for u in range(2):
            parts = []
            for t in range(n_tp):
                for j in range(n_sp // 4):
                    even = ho_buf[t, 4 * j + p].astype(f32)
                    odd = ho_buf[t, 4 * j + 2 + p].astype(f32)
                    if u == 0:
                        part = jnp.where(low_quarter, even, roll_half(odd))
                    else:
                        part = jnp.where(low_quarter, roll_half(even), odd)
                    parts.append(part.astype(bf16))
            blocks.append(jnp.concatenate(parts, axis=1))
    heads = jnp.concatenate(blocks, axis=0)
    loads[0].wait()
    attn = jnp.dot(heads, w_out[...], preferred_element_type=f32)
    hidden = (res_in[...].astype(f32) + attn).astype(bf16)
    hid_buf[me_t] = hidden

    def get_hid(t):
        return hid_buf.at[t]

    gather_start(1, get_hid)

    outgoing = jnp.dot(spread, hidden, preferred_element_type=f32).astype(bf16)
    disp_out[...] = outgoing.reshape(n_sp, cap, col_dev)
    for d in range(1, n_sp):
        sends.append(
            send(
                disp_out.at[d],
                arr_buf.at[me_t, d],
                d_send.at[d],
                d_recv.at[d],
                {"sp": lax.rem(me_s + d, n_sp)},
            )
        )
    arr_buf[me_t, 0] = disp_out[0]

    def get_arr(d):
        return lambda t: arr_buf.at[t, d]

    gather_start(2, get_arr(0))
    gather_relay(1, get_hid)

    def normalise(pieces):
        full = [piece.astype(f32) for piece in pieces]
        squares = sum(jnp.sum(piece * piece, axis=1, keepdims=True) for piece in full)
        factor = lax.rsqrt(squares * (1.0 / (n_tp * col_dev)) + epsilon)
        return jnp.concatenate(
            [
                (piece * factor * norm_g[:, t * col_dev : (t + 1) * col_dev]).astype(bf16)
                for t, piece in enumerate(full)
            ],
            axis=1,
        )

    def gated(normed, gate, up):
        gate_part = contract_last(normed, gate[...])
        up_part = contract_last(normed, up[...])
        return (gate_part / (1.0 + jnp.exp(-gate_part)) * up_part).astype(bf16)

    def arrive(d):
        wait_recv(
            arr_buf.at[me_t, d], d_send.at[d], d_recv.at[d], {"sp": lax.rem(me_s + d, n_sp)}
        )
        gather_start(2 + d, get_arr(d))
        gather_relay(1 + d, get_arr(d - 1))

    def get_sh(t):
        return sh_buf.at[t]

    def get_eh(g):
        return lambda t: eh_buf.at[t, g]

    piece_sh = 2 + n_sp
    piece_eh = 3 + n_sp

    def expert_up(g):
        ds = range(g * per_group, (g + 1) * per_group)
        for d in ds:
            gather_finish(2 + d, get_arr(d))
        normed = normalise(
            [
                arr_buf[t, g * per_group : (g + 1) * per_group].reshape(per_group * cap, col_dev)
                for t in range(n_tp)
            ]
        )
        eh_buf[me_t, g] = gated(normed, w_gate, w_up)
        gather_start(piece_eh + g, get_eh(g))

    def expert_out(g):
        gather_finish(piece_eh + g, get_eh(g))
        joined = jnp.concatenate([eh_buf[t, g] for t in range(n_tp)], axis=1)
        result = jnp.dot(joined, w_down[...], preferred_element_type=f32).astype(bf16)
        res_out[g * per_group : (g + 1) * per_group] = result.reshape(per_group, cap, col_dev)
        for d in range(g * per_group, (g + 1) * per_group):
            if d == 0:
                ret_buf[0] = res_out[0]
            else:
                sends.append(
                    send(
                        res_out.at[d],
                        ret_buf.at[d],
                        r_send.at[d],
                        r_recv.at[d],
                        {"sp": lax.rem(me_s + n_sp - d, n_sp)},
                    )
                )

    arrive(1)
    arrive(2)
    gather_finish(1, get_hid)
    loads[1].wait()
    loads[2].wait()
    normed_own = normalise([hid_buf[t] for t in range(n_tp)])
    sh_buf[me_t] = gated(normed_own, w_sgate, w_sup)
    gather_start(piece_sh, get_sh)
    for i in range(3, 7):
        loads[i].wait()
    done = 0
    for d in range(3, n_sp):
        arrive(d)
        if (d - 1) % per_group == per_group - 1 and d > per_group - 1:
            expert_up(done)
            done += 1
    gather_relay(1 + n_sp, get_arr(n_sp - 1))
    gather_relay(piece_sh, get_sh)
    for g in range(done):
        gather_relay(piece_eh + g, get_eh(g))
    for g in range(groups):
        if g == done:
            expert_up(g)
            done += 1
        if g + 1 == done and g == groups - 1:
            gather_relay(piece_eh + g, get_eh(g))
        if g + 1 == groups - 1 and done == groups - 1:
            expert_up(g + 1)
            done += 1
        expert_out(g)

    gather_finish(piece_sh, get_sh)
    shared_all = jnp.concatenate([sh_buf[t] for t in range(n_tp)], axis=1)
    result = hid_buf[me_t].astype(f32) + jnp.dot(
        shared_all, w_sdown[...], preferred_element_type=f32
    )
    col_iota = lax.broadcasted_iota(jnp.int32, (rows, slots), 1)
    picks = [
        jnp.where(col_iota == slot_col[:, c : c + 1], 1.0, 0.0).astype(bf16) for c in range(2)
    ]
    for d in range(1, n_sp):
        wait_recv(ret_buf.at[d], r_send.at[d], r_recv.at[d], {"sp": lax.rem(me_s + d, n_sp)})
    returned = ret_buf[...].reshape(slots, col_dev)
    for c in range(2):
        picked = jnp.dot(picks[c], returned, preferred_element_type=f32)
        result = result + route_w[:, c : c + 1] * picked
    out_ref[...] = result.astype(out_ref.dtype)

    for copy in sends:
        copy.wait_send()
    for s in range(n_sp):

        @pl.when(me_s != s)
        def _():
            pltpu.make_async_remote_copy(
                src_ref=o_out.at[s],
                dst_ref=ho_buf.at[me_t, me_s],
                send_sem=o_send.at[s],
                recv_sem=o_recv.at[me_s],
                device_id={"sp": s},
                device_id_type=MESH,
            ).wait_send()


def fused_body(
    residual_in,
    query_rows,
    key_rows,
    value_rows,
    map_weight,
    head_gain,
    out_proj,
    norm_gain,
    route_ids,
    route_weights,
    expert_gate,
    expert_up,
    expert_down,
    shared_gate,
    shared_up,
    shared_down,
):
    n_sp = lax.axis_size("sp")
    n_tp = lax.axis_size("tp")
    rows, col_dev = residual_in.shape
    topk = route_ids.shape[1]
    capacity = 5 * rows * topk // (4 * n_sp)
    cap = (capacity + 15) // 16 * 16
    hid_units = shared_gate.shape[0]
    width = shared_gate.shape[1]
    me_s = lax.axis_index("sp")
    flat = route_ids.reshape(-1)
    order = jnp.arange(flat.shape[0], dtype=jnp.int32)
    same = (flat[:, None] == flat[None, :]) & (order[None, :] < order[:, None])
    position = jnp.sum(same.astype(jnp.int32), axis=1)
    place = lax.rem(flat - me_s + n_sp, n_sp)
    slot_col = (place * cap + position).reshape(rows, topk)
    slot_row = slot_col.T
    map_vec = jnp.broadcast_to(
        lax.dynamic_slice_in_dim(map_weight, me_s // 2, 1)[None, :], (1, 128)
    )
    gain_vec = jnp.concatenate([jnp.zeros((64,), jnp.float32), head_gain])[None, :]
    bf16 = jnp.bfloat16
    groups = 2
    pieces = 3 + n_sp + groups
    n_gs = 1 + 2 * (n_tp // 2 - 1)
    dma = pltpu.SemaphoreType.DMA
    vmem = pl.BlockSpec(memory_space=pltpu.VMEM)
    hbm = pl.BlockSpec(memory_space=pl.ANY)
    return pl.pallas_call(
        functools.partial(layer_kernel, n_sp, n_tp),
        out_shape=jax.ShapeDtypeStruct((rows, col_dev), bf16),
        in_specs=[vmem] * 10 + [hbm] * 7,
        out_specs=vmem,
        scratch_shapes=[
            pltpu.VMEM(out_proj.shape, bf16),
            pltpu.VMEM(expert_gate.shape[1:], bf16),
            pltpu.VMEM(expert_up.shape[1:], bf16),
            pltpu.VMEM(expert_down.shape[1:], bf16),
            pltpu.VMEM(shared_gate.shape, bf16),
            pltpu.VMEM(shared_up.shape, bf16),
            pltpu.VMEM(shared_down.shape, bf16),
            pltpu.VMEM((n_sp // 2, rows, 128), bf16),
            pltpu.VMEM((n_sp, rows // 4, 128), bf16),
            pltpu.VMEM((n_sp, rows, 128), bf16),
            pltpu.VMEM((n_sp, rows // 4, 128), bf16),
            pltpu.VMEM((n_sp, rows // 4, 128), bf16),
            pltpu.VMEM((n_tp, n_sp, rows // 4, 128), bf16),
            pltpu.VMEM((n_tp, rows, col_dev), bf16),
            pltpu.VMEM((n_sp, cap, col_dev), bf16),
            pltpu.VMEM((n_tp, n_sp, cap, col_dev), bf16),
            pltpu.VMEM((n_tp, rows, hid_units), bf16),
            pltpu.VMEM((n_tp, groups, n_sp // groups * cap, hid_units), bf16),
            pltpu.VMEM((n_sp, cap, col_dev), bf16),
            pltpu.VMEM((n_sp, cap, col_dev), bf16),
            dma((7,)),
            dma((2 * n_sp,)),
            dma((n_sp,)),
            dma((n_sp,)),
            dma((n_sp,)),
            dma((n_sp,)),
            dma((n_sp,)),
            dma((n_sp,)),
            dma((n_sp,)),
            dma((n_sp,)),
            dma((pieces * n_gs,)),
            dma((pieces * n_tp,)),
        ],
        compiler_params=pltpu.CompilerParams(collective_id=0, has_side_effects=True),
    )(
        query_rows,
        key_rows,
        value_rows,
        residual_in,
        map_vec,
        gain_vec,
        norm_gain[None, :],
        slot_row,
        slot_col,
        route_weights,
        out_proj,
        expert_gate,
        expert_up,
        expert_down,
        shared_gate,
        shared_up,
        shared_down,
    )


def layer(*args):
    residual_in, map_weight, head_gain, route_ids = args[0], args[4], args[5], args[8]
    fits = (
        2 * map_weight.shape[0] == lax.axis_size("sp")
        and map_weight.shape[0] % 2 == 0
        and head_gain.shape[0] == 64
        and route_ids.shape[1] == 2
        and args[10].shape[0] == 1
        and residual_in.shape[0] % 64 == 0
        and residual_in.shape[1] % 128 == 0
        and args[13].shape[0] % 128 == 0
        and lax.axis_size("tp") % 2 == 0
    )
    return (fused_body if fits else body)(*args)


def solution(mesh):
    in_specs = (
        P("sp", "tp"),
        P("sp", "tp"),
        P("sp", "tp"),
        P("sp", "tp"),
        P("tp"),
        P(),
        P(None, "tp"),
        P(),
        P("sp", None),
        P("sp", None),
        P("sp", "tp", None),
        P("sp", "tp", None),
        P("sp", None, "tp"),
        P("tp", None),
        P("tp", None),
        P(None, "tp"),
    )
    out_specs = P("sp", "tp")
    return jax.shard_map(layer, mesh=mesh, in_specs=in_specs, out_specs=out_specs, check_vma=False)
```

```python
import functools

import jax
import jax.numpy as jnp
from jax import lax
from jax.experimental import pallas as pl
from jax.experimental.pallas import tpu as pltpu
from jax.sharding import PartitionSpec as P

epsilon = 1e-06
masked_score = -1e30
MESH = pl.DeviceIdType.MESH


def rms_scale(values, gain_vec):
    squares = jnp.mean(values * values, axis=-1, keepdims=True)
    return values * lax.rsqrt(squares + epsilon) * gain_vec


def block_slots(route_block, experts_all, capacity):
    flat_ids = route_block.reshape(-1)
    one_hot = (flat_ids[:, None] == jnp.arange(experts_all, dtype=jnp.int32)[None, :]).astype(
        jnp.int32
    )
    earlier = jnp.cumsum(one_hot, axis=0) - one_hot
    position = jnp.sum(earlier * one_hot, axis=1)
    return (flat_ids * capacity + position).reshape(route_block.shape)


def body(
    residual_in,
    query_rows,
    key_rows,
    value_rows,
    map_weight,
    head_gain,
    out_proj,
    norm_gain,
    route_ids,
    route_weights,
    expert_gate,
    expert_up,
    expert_down,
    shared_gate,
    shared_up,
    shared_down,
):
    seq_dev = residual_in.shape[0]
    col_dev = residual_in.shape[1]
    heads_here = map_weight.shape[0]
    head_dim = head_gain.shape[0]
    half_dim = head_dim // 2
    topk_count = route_ids.shape[1]
    exp_here = expert_gate.shape[0]
    experts_all = exp_here * lax.axis_size("sp")
    capacity = 5 * seq_dev * topk_count // (4 * experts_all)
    score_scale = half_dim ** (-0.5)
    query_pos = lax.axis_index("sp") * seq_dev + jnp.arange(seq_dev, dtype=jnp.int32)
    query_heads = query_rows.reshape(seq_dev, heads_here, 2, half_dim)
    key_piece = lax.all_gather(key_rows, "sp", axis=0, tiled=True)
    value_piece = lax.all_gather(value_rows, "sp", axis=0, tiled=True)
    piece_len = key_piece.shape[0]
    key_heads = key_piece.reshape(piece_len, heads_here, 2, half_dim)
    value_heads = value_piece.reshape(piece_len, heads_here, head_dim)
    scores = (
        jnp.einsum("qhmd,khmd->mhqk", query_heads, key_heads, preferred_element_type=jnp.float32)
        * score_scale
    )
    key_pos = jnp.arange(piece_len, dtype=jnp.int32)
    visible = key_pos[None, :] <= query_pos[:, None]
    scores = jnp.where(visible, scores, masked_score)
    run_max = jnp.full((2, heads_here, seq_dev), masked_score, jnp.float32)
    new_max = jnp.maximum(run_max, jnp.max(scores, axis=-1))
    expo = jnp.where(visible, jnp.exp(scores - new_max[..., None]), 0.0)
    new_sum = jnp.sum(expo, axis=-1)
    product = jnp.einsum(
        "mhqk,khd->mhqd", expo.astype(jnp.bfloat16), value_heads, preferred_element_type=jnp.float32
    )
    summed = product / new_sum[..., None]
    diff_out = summed[0] - map_weight[:, None, None] * summed[1]
    head_out = rms_scale(diff_out, head_gain).astype(jnp.bfloat16)
    head_out = jnp.transpose(head_out, (1, 0, 2)).reshape(seq_dev, heads_here * head_dim)
    attn = jnp.dot(
        lax.all_gather(head_out, "tp", axis=1, tiled=True),
        out_proj,
        preferred_element_type=jnp.float32,
    )
    hidden_state = (residual_in.astype(jnp.float32) + attn).astype(jnp.bfloat16)
    full_rows = lax.all_gather(hidden_state, "tp", axis=1, tiled=True)
    normed = rms_scale(full_rows.astype(jnp.float32), norm_gain).astype(jnp.bfloat16)
    shared_gate_part = jnp.einsum(
        "rd,fd->rf", normed, shared_gate, preferred_element_type=jnp.float32
    )
    shared_up_part = jnp.einsum("rd,fd->rf", normed, shared_up, preferred_element_type=jnp.float32)
    shared_hidden = (jax.nn.silu(shared_gate_part) * shared_up_part).astype(jnp.bfloat16)
    slot_ids = block_slots(route_ids, experts_all, capacity)
    token_of = jnp.repeat(jnp.arange(seq_dev, dtype=jnp.int32), topk_count)
    slot_token = (
        jnp.full((experts_all * capacity,), seq_dev, jnp.int32)
        .at[slot_ids.reshape(-1)]
        .set(token_of)
    )
    own_cols = lax.dynamic_slice_in_dim(normed, lax.axis_index("tp") * col_dev, col_dev, 1)
    padded = jnp.concatenate([own_cols, jnp.zeros((1, col_dev), jnp.bfloat16)], axis=0)
    outgoing = jnp.take(padded, slot_token, axis=0).reshape(experts_all, capacity, col_dev)
    arrived = lax.all_to_all(outgoing, "sp", split_axis=0, concat_axis=1, tiled=True)
    arrived_rows = arrived.shape[1]
    pieces = lax.all_gather(arrived, "tp", axis=2, tiled=True)
    gate_add = jnp.einsum("erd,efd->erf", pieces, expert_gate, preferred_element_type=jnp.float32)
    up_add = jnp.einsum("erd,efd->erf", pieces, expert_up, preferred_element_type=jnp.float32)
    expert_hidden = (jax.nn.silu(gate_add) * up_add).astype(jnp.bfloat16)
    expert_flat = expert_hidden.reshape(exp_here * arrived_rows, expert_hidden.shape[2])
    pieces = (
        lax.all_gather(shared_hidden, "tp", axis=1, tiled=True),
        lax.all_gather(expert_flat, "tp", axis=1, tiled=True),
    )
    piece_width = pieces[0].shape[1]
    routed_piece = pieces[1].reshape(exp_here, arrived_rows, piece_width)
    shared_add = jnp.dot(pieces[0], shared_down, preferred_element_type=jnp.float32)
    expert_add = jnp.einsum(
        "erf,efd->erd", routed_piece, expert_down, preferred_element_type=jnp.float32
    )
    returned_rows = lax.all_to_all(
        expert_add.astype(jnp.bfloat16), "sp", split_axis=1, concat_axis=0, tiled=True
    )
    returned_flat = returned_rows.reshape(experts_all * capacity, col_dev)
    picked = (
        jnp.take(returned_flat, slot_ids.reshape(-1), axis=0)
        .reshape(seq_dev, topk_count, col_dev)
        .astype(jnp.float32)
    )
    routed = jnp.sum(picked * route_weights[:, :, None], axis=1)
    return (hidden_state.astype(jnp.float32) + shared_add + routed).astype(jnp.bfloat16)


def lane_iota(rows):
    return lax.broadcasted_iota(jnp.int32, (rows, 128), 1)


def roll_half(values):
    return pltpu.roll(values, 64, 1)


def contract_last(a, b):
    return lax.dot_general(a, b, (((1,), (1,)), ((), ())), preferred_element_type=jnp.float32)


def layer_kernel(
    n_sp,
    n_tp,
    q_in,
    k_in,
    v_in,
    res_in,
    map_w,
    head_g,
    norm_g,
    ids_in,
    route_w,
    out_proj,
    exp_gate,
    exp_up,
    exp_down,
    sh_gate,
    sh_up,
    sh_down,
    out_ref,
    w_out,
    w_gate,
    w_up,
    w_down,
    w_sgate,
    w_sup,
    w_sdown,
    kv_out,
    q_out,
    kv_buf,
    q_buf,
    o_out,
    ho_buf,
    hid_buf,
    disp_out,
    arr_buf,
    sh_buf,
    eh_buf,
    res_out,
    ret_buf,
    spread_buf,
    pick_buf,
    weight_buf,
    w_sem,
    a_send,
    kv_recv,
    q_recv,
    o_send,
    o_recv,
    d_send,
    d_recv,
    r_send,
    r_recv,
    g_send,
    g_recv,
):
    me_s = lax.axis_index("sp")
    me_t = lax.axis_index("tp")
    sib = me_t + 1 - 2 * lax.rem(me_t, 2)
    peers = n_tp // 2 - 1
    rows = res_in.shape[0]
    col_dev = res_in.shape[1]
    half = rows // 2
    quarter = rows // 4
    cap = arr_buf.shape[2]
    half_dim = 32
    groups = eh_buf.shape[1]
    per_group = n_sp // groups
    bf16 = jnp.bfloat16
    f32 = jnp.float32

    def across(k):
        other = me_s
        for b in range(n_sp.bit_length() - 1):
            if k >> b & 1:
                bit = lax.rem(me_s // (1 << b), 2)
                other = other + (1 << b) * (1 - 2 * bit)
        return other

    loads = []
    for i, (src, dst) in enumerate(
        (
            (out_proj, w_out),
            (sh_gate, w_sgate),
            (sh_up, w_sup),
            (exp_gate.at[0], w_gate),
            (exp_up.at[0], w_up),
            (exp_down.at[0], w_down),
            (sh_down, w_sdown),
        )
    ):
        copy = pltpu.make_async_copy(src, dst, w_sem.at[i])
        copy.start()
        loads.append(copy)

    barrier = pltpu.get_barrier_semaphore()
    for d in range(1, n_sp):
        pl.semaphore_signal(
            barrier, inc=1, device_id={"sp": lax.rem(me_s + d, n_sp)}, device_id_type=MESH
        )
    for d in range(1, n_tp):
        pl.semaphore_signal(
            barrier, inc=1, device_id={"tp": lax.rem(me_t + d, n_tp)}, device_id_type=MESH
        )

    sends = []

    def send(src, dst, ssem, rsem, device):
        copy = pltpu.make_async_remote_copy(
            src_ref=src,
            dst_ref=dst,
            send_sem=ssem,
            recv_sem=rsem,
            device_id=device,
            device_id_type=MESH,
        )
        copy.start()
        return copy

    def wait_recv(ref, ssem, rsem, device):
        pltpu.make_async_remote_copy(
            src_ref=ref,
            dst_ref=ref,
            send_sem=ssem,
            recv_sem=rsem,
            device_id=device,
            device_id_type=MESH,
        ).wait_recv()

    n_gs = 1 + 2 * peers

    def gather_start(piece, get):
        for k in range(1, peers + 1):
            other = lax.rem(me_t + 2 * k, n_tp)
            sends.append(
                send(
                    get(me_t),
                    get(me_t),
                    g_send.at[piece * n_gs + k],
                    g_recv.at[piece * n_tp + me_t],
                    {"tp": other},
                )
            )
        sends.append(
            send(
                get(me_t),
                get(me_t),
                g_send.at[piece * n_gs],
                g_recv.at[piece * n_tp + me_t],
                {"tp": sib},
            )
        )

    def gather_relay(piece, get):
        for k in range(1, peers + 1):
            other = lax.rem(me_t + 2 * k, n_tp)
            wait_recv(
                get(other), g_send.at[piece * n_gs], g_recv.at[piece * n_tp + other], {"tp": sib}
            )
            sends.append(
                send(
                    get(other),
                    get(other),
                    g_send.at[piece * n_gs + peers + k],
                    g_recv.at[piece * n_tp + other],
                    {"tp": sib},
                )
            )

    def gather_finish(piece, get):
        for k in range(peers + 1):
            other = lax.rem(sib + 2 * k, n_tp)
            wait_recv(
                get(other), g_send.at[piece * n_gs], g_recv.at[piece * n_tp + other], {"tp": sib}
            )

    low_rows = lane_iota(rows) < 64
    low_quarter = lane_iota(quarter) < 64
    for j in range(n_sp // 4):
        pair = slice(j * 128, (j + 1) * 128)
        keys = k_in[:, pair].astype(f32)
        vals = v_in[:, pair].astype(f32)
        kv_out[2 * j] = jnp.where(low_rows, keys, roll_half(vals)).astype(bf16)
        kv_out[2 * j + 1] = jnp.where(low_rows, roll_half(keys), vals).astype(bf16)
        for p in range(2):
            first = q_in[p * half : p * half + quarter, pair].astype(f32)
            second = q_in[p * half + quarter : (p + 1) * half, pair].astype(f32)
            q_out[4 * j + p] = jnp.where(low_quarter, first, roll_half(second)).astype(bf16)
            q_out[4 * j + 2 + p] = jnp.where(low_quarter, roll_half(first), second).astype(bf16)

    pl.semaphore_wait(barrier, n_sp + n_tp - 2)

    for d in range(1, n_sp):
        dst = across(d)
        sends.append(
            send(
                kv_out.at[dst // 2],
                kv_buf.at[me_s],
                a_send.at[2 * d],
                kv_recv.at[me_s],
                {"sp": dst},
            )
        )
        sends.append(
            send(
                q_out.at[dst], q_buf.at[me_s], a_send.at[2 * d + 1], q_recv.at[me_s], {"sp": dst}
            )
        )
    kv_buf[me_s] = kv_out[me_s // 2]
    q_buf[me_s] = q_out[me_s]

    eye = lax.broadcasted_iota(jnp.int32, (rows, rows), 0)
    eye_lane = lax.broadcasted_iota(jnp.int32, (rows, rows), 1)
    same = eye == eye_lane
    before_col = eye_lane < eye
    before_row = eye < eye_lane

    def as_column(row):
        return jnp.sum(jnp.where(same, row, 0.0), axis=1, keepdims=True)

    ids_row = [jnp.bitwise_xor(ids_in[c : c + 1, :], me_s).astype(f32) for c in range(2)]
    ids_col = [as_column(row) for row in ids_row]
    weight_col = [as_column(route_w[c : c + 1, :]) for c in range(2)]
    slot_row = []
    slot_col = []
    for c in range(2):
        hit = (ids_row[0] == ids_col[c]) | (ids_row[1] == ids_col[c])
        count = jnp.sum(jnp.where(hit & before_col, 1.0, 0.0), axis=1, keepdims=True)
        slot_col.append(ids_col[c] * cap + count)
        hit = (ids_col[0] == ids_row[c]) | (ids_col[1] == ids_row[c])
        count = jnp.sum(jnp.where(hit & before_row, 1.0, 0.0), axis=0, keepdims=True)
        slot_row.append(ids_row[c] * cap + count)
    slots = n_sp * cap
    slot_iota = lax.broadcasted_iota(jnp.int32, (slots, rows), 0).astype(f32)
    chosen = (slot_iota == slot_row[0]) | (slot_iota == slot_row[1])
    spread_buf[...] = jnp.where(chosen, 1.0, 0.0).astype(bf16)
    col_iota = lax.broadcasted_iota(jnp.int32, (rows, slots), 1).astype(f32)
    for c in range(2):
        pick_buf[c] = jnp.where(col_iota == slot_col[c], 1.0, 0.0).astype(bf16)
        weight_buf[c] = jnp.broadcast_to(weight_col[c], (rows, 128))
    head_lane = lax.broadcasted_iota(jnp.int32, map_w.shape, 1)
    map_here = jnp.sum(
        jnp.where(head_lane == me_s // 2, map_w[...], 0.0), axis=1, keepdims=True
    )
    gain_here = jnp.concatenate([jnp.zeros((1, 64), f32), head_g[...]], axis=1)

    parity = lax.rem(me_s, 2)
    lane_q = lane_iota(quarter)
    scale = half_dim ** (-0.5)
    row_in = lax.broadcasted_iota(jnp.int32, (half, rows), 0) + parity * half
    visible_half = lax.broadcasted_iota(jnp.int32, (half, rows), 1) <= row_in
    visible = jnp.concatenate([visible_half.astype(f32)] * 2, axis=0) > 0.5
    high_lanes = lane_iota(half) >= 64
    zero_q = jnp.zeros((quarter, 128), f32)
    for s in range(n_sp):

        @pl.when(me_s != s)
        def _():
            wait_recv(kv_buf.at[s], a_send.at[0], kv_recv.at[s], {"sp": s})
            wait_recv(q_buf.at[s], a_send.at[1], q_recv.at[s], {"sp": s})

        packed = q_buf[s].astype(f32)
        rolled = roll_half(packed)
        first_map = lane_q < 32
        second_map = (lane_q >= 32) & (lane_q < 64)
        queries = jnp.concatenate(
            [
                jnp.where(first_map, packed, zero_q),
                jnp.where(first_map, rolled, zero_q),
                jnp.where(second_map, packed, zero_q),
                jnp.where(second_map, rolled, zero_q),
            ],
            axis=0,
        ).astype(bf16)
        diag = contract_last(queries, kv_buf[s]) * scale
        diag = jnp.where(visible, diag, masked_score)
        row_max = jnp.max(diag, axis=1, keepdims=True)
        if s:
            before = kv_buf[0:s].reshape(s * rows, 128)
            early = contract_last(queries, before) * scale
            row_max = jnp.maximum(row_max, jnp.max(early, axis=1, keepdims=True))
        expo = jnp.where(visible, jnp.exp(diag - row_max), 0.0)
        total = jnp.sum(expo, axis=1, keepdims=True)
        acc = jnp.dot(expo.astype(bf16), kv_buf[s], preferred_element_type=f32)
        if s:
            expo_early = jnp.exp(early - row_max)
            total = total + jnp.sum(expo_early, axis=1, keepdims=True)
            acc = acc + jnp.dot(expo_early.astype(bf16), before, preferred_element_type=f32)
        summed = acc / total
        diff = summed[0:half] - map_here * summed[half:rows]
        diff = jnp.where(high_lanes, diff, 0.0)
        squares = jnp.sum(diff * diff, axis=1, keepdims=True) * (1.0 / 64.0)
        head = diff * lax.rsqrt(squares + epsilon) * gain_here
        o_out[s] = (roll_half(head[0:quarter]) + head[quarter:half]).astype(bf16)

        @pl.when(me_s != s)
        def _():
            send(
                o_out.at[s],
                ho_buf.at[me_t, me_s],
                o_send.at[s],
                o_recv.at[me_s],
                {"sp": s},
            )

        @pl.when(me_s == s)
        def _():
            ho_buf[me_t, s] = o_out[s]

    split = n_sp // 2
    near = me_s // split * split

    def get_near(t):
        return ho_buf.at[t, pl.ds(near, split)]

    def get_far(t):
        return ho_buf.at[t, pl.ds(split - near, split)]

    for d in range(1, n_sp):
        if d == split:
            gather_start(0, get_near)
        other = across(d)
        wait_recv(ho_buf.at[me_t, other], o_send.at[d], o_recv.at[other], {"sp": other})
    gather_start(3 + n_sp + groups, get_far)
    for piece, get in ((0, get_near), (3 + n_sp + groups, get_far)):
        gather_relay(piece, get)
    for piece, get in ((0, get_near), (3 + n_sp + groups, get_far)):
        gather_finish(piece, get)

    blocks = []
    for p in range(2):
        for u in range(2):
            parts = []
            for t in range(n_tp):
                for j in range(n_sp // 4):
                    even = ho_buf[t, 4 * j + p].astype(f32)
                    odd = ho_buf[t, 4 * j + 2 + p].astype(f32)
                    if u == 0:
                        part = jnp.where(low_quarter, even, roll_half(odd))
                    else:
                        part = jnp.where(low_quarter, roll_half(even), odd)
                    parts.append(part.astype(bf16))
            blocks.append(jnp.concatenate(parts, axis=1))
    heads = jnp.concatenate(blocks, axis=0)
    loads[0].wait()
    attn = jnp.dot(heads, w_out[...], preferred_element_type=f32)
    hidden = (res_in[...].astype(f32) + attn).astype(bf16)
    hid_buf[me_t] = hidden

    def get_hid(t):
        return hid_buf.at[t]

    gather_start(1, get_hid)

    outgoing = jnp.dot(spread_buf[cap:slots], hidden, preferred_element_type=f32).astype(bf16)
    disp_out[1:n_sp] = outgoing.reshape(n_sp - 1, cap, col_dev)
    for d in range(1, n_sp):
        sends.append(
            send(
                disp_out.at[d],
                arr_buf.at[me_t, d],
                d_send.at[d],
                d_recv.at[d],
                {"sp": across(d)},
            )
        )

    def get_arr(d):
        return lambda t: arr_buf.at[t, d]

    def normalise(pieces):
        full = [piece.astype(f32) for piece in pieces]
        squares = sum(jnp.sum(piece * piece, axis=1, keepdims=True) for piece in full)
        factor = lax.rsqrt(squares * (1.0 / (n_tp * col_dev)) + epsilon)
        return jnp.concatenate(
            [
                (piece * factor * norm_g[:, t * col_dev : (t + 1) * col_dev]).astype(bf16)
                for t, piece in enumerate(full)
            ],
            axis=1,
        )

    def gated(normed, gate, up):
        gate_part = contract_last(normed, gate[...])
        up_part = contract_last(normed, up[...])
        return (gate_part / (1.0 + jnp.exp(-gate_part)) * up_part).astype(bf16)

    def arrive(d):
        wait_recv(arr_buf.at[me_t, d], d_send.at[d], d_recv.at[d], {"sp": across(d)})
        gather_start(2 + d, get_arr(d))

    def relay(d):
        gather_relay(2 + d, get_arr(d))

    def get_sh(t):
        return sh_buf.at[t]

    def get_eh(g):
        return lambda t: eh_buf.at[t, g]

    piece_sh = 2 + n_sp
    piece_eh = 3 + n_sp

    def expert_up(g):
        ds = range(g * per_group, (g + 1) * per_group)
        for d in ds:
            if d:
                gather_finish(2 + d, get_arr(d))
        normed = normalise(
            [
                arr_buf[t, g * per_group : (g + 1) * per_group].reshape(per_group * cap, col_dev)
                for t in range(n_tp)
            ]
        )
        eh_buf[me_t, g] = gated(normed, w_gate, w_up)
        gather_start(piece_eh + g, get_eh(g))

    def expert_out(g):
        gather_finish(piece_eh + g, get_eh(g))
        joined = jnp.concatenate([eh_buf[t, g] for t in range(n_tp)], axis=1)
        result = jnp.dot(joined, w_down[...], preferred_element_type=f32).astype(bf16)
        res_out[g * per_group : (g + 1) * per_group] = result.reshape(per_group, cap, col_dev)
        for d in range(g * per_group, (g + 1) * per_group):
            if d == 0:
                ret_buf[0] = res_out[0]
            else:
                sends.append(
                    send(
                        res_out.at[d],
                        ret_buf.at[d],
                        r_send.at[d],
                        r_recv.at[d],
                        {"sp": across(d)},
                    )
                )

    def relay_eh(g):
        gather_relay(piece_eh + g, get_eh(g))

    arrive(1)
    arrive(2)
    gather_relay(1, get_hid)
    arrive(3)
    relay(1)
    relay(2)
    gather_finish(1, get_hid)
    loads[1].wait()
    loads[2].wait()
    normed_own = normalise([hid_buf[t] for t in range(n_tp)])
    sh_buf[me_t] = gated(normed_own, w_sgate, w_sup)
    for t in range(n_tp):
        arr_buf[t, 0] = jnp.dot(
            spread_buf[0:cap], hid_buf[t], preferred_element_type=f32
        ).astype(bf16)
    for i in range(3, 7):
        loads[i].wait()
    for d in range(4, n_sp):
        arrive(d)
        relay(d - 1)
        if d % 2:
            expert_up((d - 5) // 2)
    expert_up(groups - 2)
    for g in range(groups - 2):
        relay_eh(g)
    for g in range(groups - 2):
        expert_out(g)
    relay(n_sp - 1)
    relay_eh(groups - 2)
    expert_up(groups - 1)
    expert_out(groups - 2)
    gather_start(piece_sh, get_sh)
    relay_eh(groups - 1)
    gather_relay(piece_sh, get_sh)
    expert_out(groups - 1)

    gather_finish(piece_sh, get_sh)
    shared_all = jnp.concatenate([sh_buf[t] for t in range(n_tp)], axis=1)
    result = hid_buf[me_t].astype(f32) + jnp.dot(
        shared_all, w_sdown[...], preferred_element_type=f32
    )
    for d in range(1, n_sp):
        wait_recv(ret_buf.at[d], r_send.at[d], r_recv.at[d], {"sp": across(d)})
    returned = ret_buf[...].reshape(slots, col_dev)
    for c in range(2):
        picked = jnp.dot(pick_buf[c], returned, preferred_element_type=f32)
        result = result + weight_buf[c][:, 0:1] * picked
    out_ref[...] = result.astype(out_ref.dtype)

    for copy in sends:
        copy.wait_send()
    for s in range(n_sp):

        @pl.when(me_s != s)
        def _():
            pltpu.make_async_remote_copy(
                src_ref=o_out.at[s],
                dst_ref=ho_buf.at[me_t, me_s],
                send_sem=o_send.at[s],
                recv_sem=o_recv.at[me_s],
                device_id={"sp": s},
                device_id_type=MESH,
            ).wait_send()


def fused_body(
    residual_in,
    query_rows,
    key_rows,
    value_rows,
    map_weight,
    head_gain,
    out_proj,
    norm_gain,
    route_ids,
    route_weights,
    expert_gate,
    expert_up,
    expert_down,
    shared_gate,
    shared_up,
    shared_down,
):
    n_sp = lax.axis_size("sp")
    n_tp = lax.axis_size("tp")
    rows, col_dev = residual_in.shape
    topk = route_ids.shape[1]
    capacity = 5 * rows * topk // (4 * n_sp)
    cap = (capacity + 15) // 16 * 16
    hid_units = shared_gate.shape[0]
    bf16 = jnp.bfloat16
    groups = n_sp // 2
    pieces = 4 + n_sp + groups
    n_gs = 1 + 2 * (n_tp // 2 - 1)
    dma = pltpu.SemaphoreType.DMA
    vmem = pl.BlockSpec(memory_space=pltpu.VMEM)
    hbm = pl.BlockSpec(memory_space=pl.ANY)
    return pl.pallas_call(
        functools.partial(layer_kernel, n_sp, n_tp),
        out_shape=jax.ShapeDtypeStruct((rows, col_dev), bf16),
        in_specs=[vmem] * 9 + [hbm] * 7,
        out_specs=vmem,
        scratch_shapes=[
            pltpu.VMEM(out_proj.shape, bf16),
            pltpu.VMEM(expert_gate.shape[1:], bf16),
            pltpu.VMEM(expert_up.shape[1:], bf16),
            pltpu.VMEM(expert_down.shape[1:], bf16),
            pltpu.VMEM(shared_gate.shape, bf16),
            pltpu.VMEM(shared_up.shape, bf16),
            pltpu.VMEM(shared_down.shape, bf16),
            pltpu.VMEM((n_sp // 2, rows, 128), bf16),
            pltpu.VMEM((n_sp, rows // 4, 128), bf16),
            pltpu.VMEM((n_sp, rows, 128), bf16),
            pltpu.VMEM((n_sp, rows // 4, 128), bf16),
            pltpu.VMEM((n_sp, rows // 4, 128), bf16),
            pltpu.VMEM((n_tp, n_sp, rows // 4, 128), bf16),
            pltpu.VMEM((n_tp, rows, col_dev), bf16),
            pltpu.VMEM((n_sp, cap, col_dev), bf16),
            pltpu.VMEM((n_tp, n_sp, cap, col_dev), bf16),
            pltpu.VMEM((n_tp, rows, hid_units), bf16),
            pltpu.VMEM((n_tp, groups, n_sp // groups * cap, hid_units), bf16),
            pltpu.VMEM((n_sp, cap, col_dev), bf16),
            pltpu.VMEM((n_sp, cap, col_dev), bf16),
            pltpu.VMEM((n_sp * cap, rows), bf16),
            pltpu.VMEM((2, rows, n_sp * cap), bf16),
            pltpu.VMEM((2, rows, 128), jnp.float32),
            dma((7,)),
            dma((2 * n_sp,)),
            dma((n_sp,)),
            dma((n_sp,)),
            dma((n_sp,)),
            dma((n_sp,)),
            dma((n_sp,)),
            dma((n_sp,)),
            dma((n_sp,)),
            dma((n_sp,)),
            dma((pieces * n_gs,)),
            dma((pieces * n_tp,)),
        ],
        compiler_params=pltpu.CompilerParams(collective_id=0, has_side_effects=True),
    )(
        query_rows,
        key_rows,
        value_rows,
        residual_in,
        map_weight[None, :],
        head_gain[None, :],
        norm_gain[None, :],
        route_ids.T,
        route_weights.T,
        out_proj,
        expert_gate,
        expert_up,
        expert_down,
        shared_gate,
        shared_up,
        shared_down,
    )


def layer(*args):
    residual_in, map_weight, head_gain, route_ids = args[0], args[4], args[5], args[8]
    fits = (
        2 * map_weight.shape[0] == lax.axis_size("sp") == 8
        and map_weight.shape[0] % 2 == 0
        and head_gain.shape[0] == 64
        and route_ids.shape[1] == 2
        and args[10].shape[0] == 1
        and residual_in.shape[0] % 64 == 0
        and residual_in.shape[1] % 128 == 0
        and args[13].shape[0] % 128 == 0
        and lax.axis_size("tp") % 2 == 0
    )
    return (fused_body if fits else body)(*args)


def solution(mesh):
    in_specs = (
        P("sp", "tp"),
        P("sp", "tp"),
        P("sp", "tp"),
        P("sp", "tp"),
        P("tp"),
        P(),
        P(None, "tp"),
        P(),
        P("sp", None),
        P("sp", None),
        P("sp", "tp", None),
        P("sp", "tp", None),
        P("sp", None, "tp"),
        P("tp", None),
        P("tp", None),
        P(None, "tp"),
    )
    out_specs = P("sp", "tp")
    return jax.shard_map(layer, mesh=mesh, in_specs=in_specs, out_specs=out_specs, check_vma=False)
```

```python
import functools

import jax
import jax.numpy as jnp
from jax import lax
from jax.experimental import pallas as pl
from jax.experimental.pallas import tpu as pltpu
from jax.sharding import PartitionSpec as P

epsilon = 1e-06
masked_score = -1e30
MESH = pl.DeviceIdType.MESH


def rms_scale(values, gain_vec):
    squares = jnp.mean(values * values, axis=-1, keepdims=True)
    return values * lax.rsqrt(squares + epsilon) * gain_vec


def block_slots(route_block, experts_all, capacity):
    flat_ids = route_block.reshape(-1)
    one_hot = (flat_ids[:, None] == jnp.arange(experts_all, dtype=jnp.int32)[None, :]).astype(
        jnp.int32
    )
    earlier = jnp.cumsum(one_hot, axis=0) - one_hot
    position = jnp.sum(earlier * one_hot, axis=1)
    return (flat_ids * capacity + position).reshape(route_block.shape)


def body(
    residual_in,
    query_rows,
    key_rows,
    value_rows,
    map_weight,
    head_gain,
    out_proj,
    norm_gain,
    route_ids,
    route_weights,
    expert_gate,
    expert_up,
    expert_down,
    shared_gate,
    shared_up,
    shared_down,
):
    seq_dev = residual_in.shape[0]
    col_dev = residual_in.shape[1]
    heads_here = map_weight.shape[0]
    head_dim = head_gain.shape[0]
    half_dim = head_dim // 2
    topk_count = route_ids.shape[1]
    exp_here = expert_gate.shape[0]
    experts_all = exp_here * lax.axis_size("sp")
    capacity = 5 * seq_dev * topk_count // (4 * experts_all)
    score_scale = half_dim ** (-0.5)
    query_pos = lax.axis_index("sp") * seq_dev + jnp.arange(seq_dev, dtype=jnp.int32)
    query_heads = query_rows.reshape(seq_dev, heads_here, 2, half_dim)
    key_piece = lax.all_gather(key_rows, "sp", axis=0, tiled=True)
    value_piece = lax.all_gather(value_rows, "sp", axis=0, tiled=True)
    piece_len = key_piece.shape[0]
    key_heads = key_piece.reshape(piece_len, heads_here, 2, half_dim)
    value_heads = value_piece.reshape(piece_len, heads_here, head_dim)
    scores = (
        jnp.einsum("qhmd,khmd->mhqk", query_heads, key_heads, preferred_element_type=jnp.float32)
        * score_scale
    )
    key_pos = jnp.arange(piece_len, dtype=jnp.int32)
    visible = key_pos[None, :] <= query_pos[:, None]
    scores = jnp.where(visible, scores, masked_score)
    run_max = jnp.full((2, heads_here, seq_dev), masked_score, jnp.float32)
    new_max = jnp.maximum(run_max, jnp.max(scores, axis=-1))
    expo = jnp.where(visible, jnp.exp(scores - new_max[..., None]), 0.0)
    new_sum = jnp.sum(expo, axis=-1)
    product = jnp.einsum(
        "mhqk,khd->mhqd", expo.astype(jnp.bfloat16), value_heads, preferred_element_type=jnp.float32
    )
    summed = product / new_sum[..., None]
    diff_out = summed[0] - map_weight[:, None, None] * summed[1]
    head_out = rms_scale(diff_out, head_gain).astype(jnp.bfloat16)
    head_out = jnp.transpose(head_out, (1, 0, 2)).reshape(seq_dev, heads_here * head_dim)
    attn = jnp.dot(
        lax.all_gather(head_out, "tp", axis=1, tiled=True),
        out_proj,
        preferred_element_type=jnp.float32,
    )
    hidden_state = (residual_in.astype(jnp.float32) + attn).astype(jnp.bfloat16)
    full_rows = lax.all_gather(hidden_state, "tp", axis=1, tiled=True)
    normed = rms_scale(full_rows.astype(jnp.float32), norm_gain).astype(jnp.bfloat16)
    shared_gate_part = jnp.einsum(
        "rd,fd->rf", normed, shared_gate, preferred_element_type=jnp.float32
    )
    shared_up_part = jnp.einsum("rd,fd->rf", normed, shared_up, preferred_element_type=jnp.float32)
    shared_hidden = (jax.nn.silu(shared_gate_part) * shared_up_part).astype(jnp.bfloat16)
    slot_ids = block_slots(route_ids, experts_all, capacity)
    token_of = jnp.repeat(jnp.arange(seq_dev, dtype=jnp.int32), topk_count)
    slot_token = (
        jnp.full((experts_all * capacity,), seq_dev, jnp.int32)
        .at[slot_ids.reshape(-1)]
        .set(token_of)
    )
    own_cols = lax.dynamic_slice_in_dim(normed, lax.axis_index("tp") * col_dev, col_dev, 1)
    padded = jnp.concatenate([own_cols, jnp.zeros((1, col_dev), jnp.bfloat16)], axis=0)
    outgoing = jnp.take(padded, slot_token, axis=0).reshape(experts_all, capacity, col_dev)
    arrived = lax.all_to_all(outgoing, "sp", split_axis=0, concat_axis=1, tiled=True)
    arrived_rows = arrived.shape[1]
    pieces = lax.all_gather(arrived, "tp", axis=2, tiled=True)
    gate_add = jnp.einsum("erd,efd->erf", pieces, expert_gate, preferred_element_type=jnp.float32)
    up_add = jnp.einsum("erd,efd->erf", pieces, expert_up, preferred_element_type=jnp.float32)
    expert_hidden = (jax.nn.silu(gate_add) * up_add).astype(jnp.bfloat16)
    expert_flat = expert_hidden.reshape(exp_here * arrived_rows, expert_hidden.shape[2])
    pieces = (
        lax.all_gather(shared_hidden, "tp", axis=1, tiled=True),
        lax.all_gather(expert_flat, "tp", axis=1, tiled=True),
    )
    piece_width = pieces[0].shape[1]
    routed_piece = pieces[1].reshape(exp_here, arrived_rows, piece_width)
    shared_add = jnp.dot(pieces[0], shared_down, preferred_element_type=jnp.float32)
    expert_add = jnp.einsum(
        "erf,efd->erd", routed_piece, expert_down, preferred_element_type=jnp.float32
    )
    returned_rows = lax.all_to_all(
        expert_add.astype(jnp.bfloat16), "sp", split_axis=1, concat_axis=0, tiled=True
    )
    returned_flat = returned_rows.reshape(experts_all * capacity, col_dev)
    picked = (
        jnp.take(returned_flat, slot_ids.reshape(-1), axis=0)
        .reshape(seq_dev, topk_count, col_dev)
        .astype(jnp.float32)
    )
    routed = jnp.sum(picked * route_weights[:, :, None], axis=1)
    return (hidden_state.astype(jnp.float32) + shared_add + routed).astype(jnp.bfloat16)


def lane_iota(rows):
    return lax.broadcasted_iota(jnp.int32, (rows, 128), 1)


def roll_half(values):
    return pltpu.roll(values, 64, 1)


def contract_last(a, b):
    return lax.dot_general(a, b, (((1,), (1,)), ((), ())), preferred_element_type=jnp.float32)


def layer_kernel(
    n_sp,
    n_tp,
    q_in,
    k_in,
    v_in,
    res_in,
    map_w,
    head_g,
    norm_g,
    ids_in,
    route_w,
    out_proj,
    exp_gate,
    exp_up,
    exp_down,
    sh_gate,
    sh_up,
    sh_down,
    out_ref,
    w_out,
    w_gate,
    w_up,
    w_down,
    w_sgate,
    w_sup,
    w_sdown,
    kv_out,
    q_out,
    kv_buf,
    q_buf,
    o_out,
    ho_buf,
    hid_buf,
    disp_out,
    arr_buf,
    sh_buf,
    eh_buf,
    res_out,
    ret_buf,
    spread_buf,
    pick_buf,
    weight_buf,
    w_sem,
    a_send,
    kv_recv,
    q_recv,
    o_send,
    o_recv,
    d_send,
    d_recv,
    r_send,
    r_recv,
    g_send,
    g_recv,
):
    me_s = lax.axis_index("sp")
    me_t = lax.axis_index("tp")
    sib = me_t + 1 - 2 * lax.rem(me_t, 2)
    peers = n_tp // 2 - 1
    rows = res_in.shape[0]
    col_dev = res_in.shape[1]
    half = rows // 2
    quarter = rows // 4
    cap = arr_buf.shape[2]
    half_dim = 32
    groups = eh_buf.shape[1]
    per_group = n_sp // groups
    bf16 = jnp.bfloat16
    f32 = jnp.float32

    def across(k):
        other = me_s
        for b in range(n_sp.bit_length() - 1):
            if k >> b & 1:
                bit = lax.rem(me_s // (1 << b), 2)
                other = other + (1 << b) * (1 - 2 * bit)
        return other

    loads = []
    for i, (src, dst) in enumerate(
        (
            (out_proj, w_out),
            (sh_gate, w_sgate),
            (sh_up, w_sup),
            (exp_gate.at[0], w_gate),
            (exp_up.at[0], w_up),
            (exp_down.at[0], w_down),
            (sh_down, w_sdown),
        )
    ):
        copy = pltpu.make_async_copy(src, dst, w_sem.at[i])
        copy.start()
        loads.append(copy)

    barrier = pltpu.get_barrier_semaphore()
    for d in range(1, n_sp):
        pl.semaphore_signal(
            barrier, inc=1, device_id={"sp": lax.rem(me_s + d, n_sp)}, device_id_type=MESH
        )
    for d in range(1, n_tp):
        pl.semaphore_signal(
            barrier, inc=1, device_id={"tp": lax.rem(me_t + d, n_tp)}, device_id_type=MESH
        )

    sends = []

    def send(src, dst, ssem, rsem, device):
        copy = pltpu.make_async_remote_copy(
            src_ref=src,
            dst_ref=dst,
            send_sem=ssem,
            recv_sem=rsem,
            device_id=device,
            device_id_type=MESH,
        )
        copy.start()
        return copy

    def wait_recv(ref, ssem, rsem, device):
        pltpu.make_async_remote_copy(
            src_ref=ref,
            dst_ref=ref,
            send_sem=ssem,
            recv_sem=rsem,
            device_id=device,
            device_id_type=MESH,
        ).wait_recv()

    n_gs = 1 + 2 * peers

    def gather_start(piece, get):
        for k in range(1, peers + 1):
            other = lax.rem(me_t + 2 * k, n_tp)
            sends.append(
                send(
                    get(me_t),
                    get(me_t),
                    g_send.at[piece * n_gs + k],
                    g_recv.at[piece * n_tp + me_t],
                    {"tp": other},
                )
            )
        sends.append(
            send(
                get(me_t),
                get(me_t),
                g_send.at[piece * n_gs],
                g_recv.at[piece * n_tp + me_t],
                {"tp": sib},
            )
        )

    def gather_relay(piece, get):
        for k in range(1, peers + 1):
            other = lax.rem(me_t + 2 * k, n_tp)
            wait_recv(
                get(other), g_send.at[piece * n_gs], g_recv.at[piece * n_tp + other], {"tp": sib}
            )
            sends.append(
                send(
                    get(other),
                    get(other),
                    g_send.at[piece * n_gs + peers + k],
                    g_recv.at[piece * n_tp + other],
                    {"tp": sib},
                )
            )

    def gather_finish(piece, get):
        for k in range(peers + 1):
            other = lax.rem(sib + 2 * k, n_tp)
            wait_recv(
                get(other), g_send.at[piece * n_gs], g_recv.at[piece * n_tp + other], {"tp": sib}
            )

    low_rows = lane_iota(rows) < 64
    low_quarter = lane_iota(quarter) < 64
    for j in range(n_sp // 4):
        pair = slice(j * 128, (j + 1) * 128)
        keys = k_in[:, pair].astype(f32)
        vals = v_in[:, pair].astype(f32)
        kv_out[2 * j] = jnp.where(low_rows, keys, roll_half(vals)).astype(bf16)
        kv_out[2 * j + 1] = jnp.where(low_rows, roll_half(keys), vals).astype(bf16)
        for p in range(2):
            first = q_in[p * half : p * half + quarter, pair].astype(f32)
            second = q_in[p * half + quarter : (p + 1) * half, pair].astype(f32)
            q_out[4 * j + p] = jnp.where(low_quarter, first, roll_half(second)).astype(bf16)
            q_out[4 * j + 2 + p] = jnp.where(low_quarter, roll_half(first), second).astype(bf16)

    pl.semaphore_wait(barrier, n_sp + n_tp - 2)

    for d in range(1, n_sp):
        dst = across(d)
        sends.append(
            send(
                kv_out.at[dst // 2],
                kv_buf.at[me_s],
                a_send.at[2 * d],
                kv_recv.at[me_s],
                {"sp": dst},
            )
        )
        sends.append(
            send(
                q_out.at[dst], q_buf.at[me_s], a_send.at[2 * d + 1], q_recv.at[me_s], {"sp": dst}
            )
        )
    kv_buf[me_s] = kv_out[me_s // 2]
    q_buf[me_s] = q_out[me_s]

    eye = lax.broadcasted_iota(jnp.int32, (rows, rows), 0)
    eye_lane = lax.broadcasted_iota(jnp.int32, (rows, rows), 1)
    same = eye == eye_lane
    before_col = eye_lane < eye
    before_row = eye < eye_lane

    def as_column(row):
        return jnp.sum(jnp.where(same, row, 0.0), axis=1, keepdims=True)

    ids_row = [jnp.bitwise_xor(ids_in[c : c + 1, :], me_s).astype(f32) for c in range(2)]
    ids_col = [as_column(row) for row in ids_row]
    weight_col = [as_column(route_w[c : c + 1, :]) for c in range(2)]
    slot_row = []
    slot_col = []
    for c in range(2):
        hit = (ids_row[0] == ids_col[c]) | (ids_row[1] == ids_col[c])
        count = jnp.sum(jnp.where(hit & before_col, 1.0, 0.0), axis=1, keepdims=True)
        slot_col.append(ids_col[c] * cap + count)
        hit = (ids_col[0] == ids_row[c]) | (ids_col[1] == ids_row[c])
        count = jnp.sum(jnp.where(hit & before_row, 1.0, 0.0), axis=0, keepdims=True)
        slot_row.append(ids_row[c] * cap + count)
    slots = n_sp * cap
    slot_iota = lax.broadcasted_iota(jnp.int32, (slots, rows), 0).astype(f32)
    chosen = (slot_iota == slot_row[0]) | (slot_iota == slot_row[1])
    spread_buf[...] = jnp.where(chosen, 1.0, 0.0).astype(bf16)
    col_iota = lax.broadcasted_iota(jnp.int32, (rows, slots), 1).astype(f32)
    for c in range(2):
        pick_buf[c] = jnp.where(col_iota == slot_col[c], 1.0, 0.0).astype(bf16)
        weight_buf[c] = jnp.broadcast_to(weight_col[c], (rows, 128))
    head_lane = lax.broadcasted_iota(jnp.int32, map_w.shape, 1)
    map_here = jnp.sum(
        jnp.where(head_lane == me_s // 2, map_w[...], 0.0), axis=1, keepdims=True
    )
    gain_here = jnp.concatenate([jnp.zeros((1, 64), f32), head_g[...]], axis=1)

    parity = lax.rem(me_s, 2)
    lane_q = lane_iota(quarter)
    scale = half_dim ** (-0.5)
    row_in = lax.broadcasted_iota(jnp.int32, (half, rows), 0) + parity * half
    visible_half = lax.broadcasted_iota(jnp.int32, (half, rows), 1) <= row_in
    visible = jnp.concatenate([visible_half.astype(f32)] * 2, axis=0) > 0.5
    high_lanes = lane_iota(half) >= 64
    zero_q = jnp.zeros((quarter, 128), f32)
    for s in range(n_sp):

        @pl.when(me_s != s)
        def _():
            wait_recv(kv_buf.at[s], a_send.at[0], kv_recv.at[s], {"sp": s})
            wait_recv(q_buf.at[s], a_send.at[1], q_recv.at[s], {"sp": s})

        packed = q_buf[s].astype(f32)
        rolled = roll_half(packed)
        first_map = lane_q < 32
        second_map = (lane_q >= 32) & (lane_q < 64)
        queries = jnp.concatenate(
            [
                jnp.where(first_map, packed, zero_q),
                jnp.where(first_map, rolled, zero_q),
                jnp.where(second_map, packed, zero_q),
                jnp.where(second_map, rolled, zero_q),
            ],
            axis=0,
        ).astype(bf16)
        diag = contract_last(queries, kv_buf[s]) * scale
        diag = jnp.where(visible, diag, masked_score)
        row_max = jnp.max(diag, axis=1, keepdims=True)
        if s:
            before = kv_buf[0:s].reshape(s * rows, 128)
            early = contract_last(queries, before) * scale
            row_max = jnp.maximum(row_max, jnp.max(early, axis=1, keepdims=True))
        expo = jnp.where(visible, jnp.exp(diag - row_max), 0.0)
        total = jnp.sum(expo, axis=1, keepdims=True)
        acc = jnp.dot(expo.astype(bf16), kv_buf[s], preferred_element_type=f32)
        if s:
            expo_early = jnp.exp(early - row_max)
            total = total + jnp.sum(expo_early, axis=1, keepdims=True)
            acc = acc + jnp.dot(expo_early.astype(bf16), before, preferred_element_type=f32)
        summed = acc / total
        diff = summed[0:half] - map_here * summed[half:rows]
        diff = jnp.where(high_lanes, diff, 0.0)
        squares = jnp.sum(diff * diff, axis=1, keepdims=True) * (1.0 / 64.0)
        head = diff * lax.rsqrt(squares + epsilon) * gain_here
        o_out[s] = (roll_half(head[0:quarter]) + head[quarter:half]).astype(bf16)

        @pl.when(me_s != s)
        def _():
            send(
                o_out.at[s],
                ho_buf.at[me_t, me_s],
                o_send.at[s],
                o_recv.at[me_s],
                {"sp": s},
            )

        @pl.when(me_s == s)
        def _():
            ho_buf[me_t, s] = o_out[s]

    split = n_sp // 2
    near = me_s // split * split

    def get_near(t):
        return ho_buf.at[t, pl.ds(near, split)]

    def get_far(t):
        return ho_buf.at[t, pl.ds(split - near, split)]

    for d in range(1, n_sp):
        if d == split:
            gather_start(0, get_near)
        other = across(d)
        wait_recv(ho_buf.at[me_t, other], o_send.at[d], o_recv.at[other], {"sp": other})
    gather_start(3 + n_sp + groups, get_far)
    for piece, get in ((0, get_near), (3 + n_sp + groups, get_far)):
        gather_relay(piece, get)
    for piece, get in ((0, get_near), (3 + n_sp + groups, get_far)):
        gather_finish(piece, get)

    blocks = []
    for p in range(2):
        for u in range(2):
            parts = []
            for t in range(n_tp):
                for j in range(n_sp // 4):
                    even = ho_buf[t, 4 * j + p].astype(f32)
                    odd = ho_buf[t, 4 * j + 2 + p].astype(f32)
                    if u == 0:
                        part = jnp.where(low_quarter, even, roll_half(odd))
                    else:
                        part = jnp.where(low_quarter, roll_half(even), odd)
                    parts.append(part.astype(bf16))
            blocks.append(jnp.concatenate(parts, axis=1))
    heads = jnp.concatenate(blocks, axis=0)
    loads[0].wait()
    attn = jnp.dot(heads, w_out[...], preferred_element_type=f32)
    hidden = (res_in[...].astype(f32) + attn).astype(bf16)
    hid_buf[me_t] = hidden

    def get_hid(t):
        return hid_buf.at[t]

    gather_start(1, get_hid)

    outgoing = jnp.dot(spread_buf[cap:slots], hidden, preferred_element_type=f32).astype(bf16)
    disp_out[1:n_sp] = outgoing.reshape(n_sp - 1, cap, col_dev)
    for d in range(1, n_sp):
        sends.append(
            send(
                disp_out.at[d],
                arr_buf.at[me_t, d],
                d_send.at[d],
                d_recv.at[d],
                {"sp": across(d)},
            )
        )

    def get_arr(d):
        return lambda t: arr_buf.at[t, d]

    def normalise(pieces):
        full = [piece.astype(f32) for piece in pieces]
        squares = sum(jnp.sum(piece * piece, axis=1, keepdims=True) for piece in full)
        factor = lax.rsqrt(squares * (1.0 / (n_tp * col_dev)) + epsilon)
        return jnp.concatenate(
            [
                (piece * factor * norm_g[:, t * col_dev : (t + 1) * col_dev]).astype(bf16)
                for t, piece in enumerate(full)
            ],
            axis=1,
        )

    def gated(normed, gate, up):
        gate_part = contract_last(normed, gate[...])
        up_part = contract_last(normed, up[...])
        return (gate_part / (1.0 + jnp.exp(-gate_part)) * up_part).astype(bf16)

    def arrive(d):
        wait_recv(arr_buf.at[me_t, d], d_send.at[d], d_recv.at[d], {"sp": across(d)})
        gather_start(2 + d, get_arr(d))

    def relay(d):
        gather_relay(2 + d, get_arr(d))

    def get_sh(t):
        return sh_buf.at[t]

    def get_eh(g):
        return lambda t: eh_buf.at[t, g]

    piece_sh = 2 + n_sp
    piece_eh = 3 + n_sp

    def expert_up(g):
        ds = range(g * per_group, (g + 1) * per_group)
        for d in ds:
            if d:
                gather_finish(2 + d, get_arr(d))
        normed = normalise(
            [
                arr_buf[t, g * per_group : (g + 1) * per_group].reshape(per_group * cap, col_dev)
                for t in range(n_tp)
            ]
        )
        eh_buf[me_t, g] = gated(normed, w_gate, w_up)

    def expert_out(g):
        gather_finish(piece_eh + g, get_eh(g))
        joined = jnp.concatenate([eh_buf[t, g] for t in range(n_tp)], axis=1)
        result = jnp.dot(joined, w_down[...], preferred_element_type=f32).astype(bf16)
        res_out[g * per_group : (g + 1) * per_group] = result.reshape(per_group, cap, col_dev)
        for d in range(g * per_group, (g + 1) * per_group):
            if d == 0:
                ret_buf[0] = res_out[0]
            else:
                sends.append(
                    send(
                        res_out.at[d],
                        ret_buf.at[d],
                        r_send.at[d],
                        r_recv.at[d],
                        {"sp": across(d)},
                    )
                )

    def relay_eh(g):
        gather_relay(piece_eh + g, get_eh(g))

    def start_eh(g):
        gather_start(piece_eh + g, get_eh(g))

    def relay_eh(g):
        gather_relay(piece_eh + g, get_eh(g))

    arrive(1)
    arrive(2)
    gather_relay(1, get_hid)
    arrive(3)
    relay(1)
    relay(2)
    arrive(4)
    gather_finish(1, get_hid)
    loads[1].wait()
    loads[2].wait()
    normed_own = normalise([hid_buf[t] for t in range(n_tp)])
    sh_buf[me_t] = gated(normed_own, w_sgate, w_sup)
    relay(3)
    arrive(5)
    relay(4)
    for t in range(n_tp):
        arr_buf[t, 0] = jnp.dot(
            spread_buf[0:cap], hid_buf[t], preferred_element_type=f32
        ).astype(bf16)
    for i in range(3, 7):
        loads[i].wait()
    expert_up(0)
    arrive(6)
    relay(5)
    expert_up(2)
    start_eh(2)
    arrive(7)
    relay(6)
    expert_up(1)
    relay_eh(2)
    relay(7)
    expert_out(2)
    expert_up(3)
    start_eh(3)
    start_eh(1)
    start_eh(0)
    gather_start(piece_sh, get_sh)
    relay_eh(3)
    expert_out(3)
    relay_eh(1)
    relay_eh(0)
    gather_relay(piece_sh, get_sh)
    expert_out(1)
    expert_out(0)

    gather_finish(piece_sh, get_sh)
    shared_all = jnp.concatenate([sh_buf[t] for t in range(n_tp)], axis=1)
    result = hid_buf[me_t].astype(f32) + jnp.dot(
        shared_all, w_sdown[...], preferred_element_type=f32
    )
    for d in range(1, n_sp):
        wait_recv(ret_buf.at[d], r_send.at[d], r_recv.at[d], {"sp": across(d)})
    returned = ret_buf[...].reshape(slots, col_dev)
    for c in range(2):
        picked = jnp.dot(pick_buf[c], returned, preferred_element_type=f32)
        result = result + weight_buf[c][:, 0:1] * picked
    out_ref[...] = result.astype(out_ref.dtype)

    for copy in sends:
        copy.wait_send()
    for s in range(n_sp):

        @pl.when(me_s != s)
        def _():
            pltpu.make_async_remote_copy(
                src_ref=o_out.at[s],
                dst_ref=ho_buf.at[me_t, me_s],
                send_sem=o_send.at[s],
                recv_sem=o_recv.at[me_s],
                device_id={"sp": s},
                device_id_type=MESH,
            ).wait_send()


def fused_body(
    residual_in,
    query_rows,
    key_rows,
    value_rows,
    map_weight,
    head_gain,
    out_proj,
    norm_gain,
    route_ids,
    route_weights,
    expert_gate,
    expert_up,
    expert_down,
    shared_gate,
    shared_up,
    shared_down,
):
    n_sp = lax.axis_size("sp")
    n_tp = lax.axis_size("tp")
    rows, col_dev = residual_in.shape
    topk = route_ids.shape[1]
    capacity = 5 * rows * topk // (4 * n_sp)
    cap = (capacity + 15) // 16 * 16
    hid_units = shared_gate.shape[0]
    bf16 = jnp.bfloat16
    groups = n_sp // 2
    pieces = 4 + n_sp + groups
    n_gs = 1 + 2 * (n_tp // 2 - 1)
    dma = pltpu.SemaphoreType.DMA
    vmem = pl.BlockSpec(memory_space=pltpu.VMEM)
    hbm = pl.BlockSpec(memory_space=pl.ANY)
    return pl.pallas_call(
        functools.partial(layer_kernel, n_sp, n_tp),
        out_shape=jax.ShapeDtypeStruct((rows, col_dev), bf16),
        in_specs=[vmem] * 9 + [hbm] * 7,
        out_specs=vmem,
        scratch_shapes=[
            pltpu.VMEM(out_proj.shape, bf16),
            pltpu.VMEM(expert_gate.shape[1:], bf16),
            pltpu.VMEM(expert_up.shape[1:], bf16),
            pltpu.VMEM(expert_down.shape[1:], bf16),
            pltpu.VMEM(shared_gate.shape, bf16),
            pltpu.VMEM(shared_up.shape, bf16),
            pltpu.VMEM(shared_down.shape, bf16),
            pltpu.VMEM((n_sp // 2, rows, 128), bf16),
            pltpu.VMEM((n_sp, rows // 4, 128), bf16),
            pltpu.VMEM((n_sp, rows, 128), bf16),
            pltpu.VMEM((n_sp, rows // 4, 128), bf16),
            pltpu.VMEM((n_sp, rows // 4, 128), bf16),
            pltpu.VMEM((n_tp, n_sp, rows // 4, 128), bf16),
            pltpu.VMEM((n_tp, rows, col_dev), bf16),
            pltpu.VMEM((n_sp, cap, col_dev), bf16),
            pltpu.VMEM((n_tp, n_sp, cap, col_dev), bf16),
            pltpu.VMEM((n_tp, rows, hid_units), bf16),
            pltpu.VMEM((n_tp, groups, n_sp // groups * cap, hid_units), bf16),
            pltpu.VMEM((n_sp, cap, col_dev), bf16),
            pltpu.VMEM((n_sp, cap, col_dev), bf16),
            pltpu.VMEM((n_sp * cap, rows), bf16),
            pltpu.VMEM((2, rows, n_sp * cap), bf16),
            pltpu.VMEM((2, rows, 128), jnp.float32),
            dma((7,)),
            dma((2 * n_sp,)),
            dma((n_sp,)),
            dma((n_sp,)),
            dma((n_sp,)),
            dma((n_sp,)),
            dma((n_sp,)),
            dma((n_sp,)),
            dma((n_sp,)),
            dma((n_sp,)),
            dma((pieces * n_gs,)),
            dma((pieces * n_tp,)),
        ],
        compiler_params=pltpu.CompilerParams(collective_id=0, has_side_effects=True),
    )(
        query_rows,
        key_rows,
        value_rows,
        residual_in,
        map_weight[None, :],
        head_gain[None, :],
        norm_gain[None, :],
        route_ids.T,
        route_weights.T,
        out_proj,
        expert_gate,
        expert_up,
        expert_down,
        shared_gate,
        shared_up,
        shared_down,
    )


def layer(*args):
    residual_in, map_weight, head_gain, route_ids = args[0], args[4], args[5], args[8]
    fits = (
        2 * map_weight.shape[0] == lax.axis_size("sp") == 8
        and map_weight.shape[0] % 2 == 0
        and head_gain.shape[0] == 64
        and route_ids.shape[1] == 2
        and args[10].shape[0] == 1
        and residual_in.shape[0] % 64 == 0
        and residual_in.shape[1] % 128 == 0
        and args[13].shape[0] % 128 == 0
        and lax.axis_size("tp") % 2 == 0
    )
    return (fused_body if fits else body)(*args)


def solution(mesh):
    in_specs = (
        P("sp", "tp"),
        P("sp", "tp"),
        P("sp", "tp"),
        P("sp", "tp"),
        P("tp"),
        P(),
        P(None, "tp"),
        P(),
        P("sp", None),
        P("sp", None),
        P("sp", "tp", None),
        P("sp", "tp", None),
        P("sp", None, "tp"),
        P("tp", None),
        P("tp", None),
        P(None, "tp"),
    )
    out_specs = P("sp", "tp")
    return jax.shard_map(layer, mesh=mesh, in_specs=in_specs, out_specs=out_specs, check_vma=False)
```

```python
import functools

import jax
import jax.numpy as jnp
from jax import lax
from jax.experimental import pallas as pl
from jax.experimental.pallas import tpu as pltpu
from jax.sharding import PartitionSpec as P

epsilon = 1e-06
masked_score = -1e30
MESH = pl.DeviceIdType.MESH


def rms_scale(values, gain_vec):
    squares = jnp.mean(values * values, axis=-1, keepdims=True)
    return values * lax.rsqrt(squares + epsilon) * gain_vec


def block_slots(route_block, experts_all, capacity):
    flat_ids = route_block.reshape(-1)
    one_hot = (flat_ids[:, None] == jnp.arange(experts_all, dtype=jnp.int32)[None, :]).astype(
        jnp.int32
    )
    earlier = jnp.cumsum(one_hot, axis=0) - one_hot
    position = jnp.sum(earlier * one_hot, axis=1)
    return (flat_ids * capacity + position).reshape(route_block.shape)


def body(
    residual_in,
    query_rows,
    key_rows,
    value_rows,
    map_weight,
    head_gain,
    out_proj,
    norm_gain,
    route_ids,
    route_weights,
    expert_gate,
    expert_up,
    expert_down,
    shared_gate,
    shared_up,
    shared_down,
):
    seq_dev = residual_in.shape[0]
    col_dev = residual_in.shape[1]
    heads_here = map_weight.shape[0]
    head_dim = head_gain.shape[0]
    half_dim = head_dim // 2
    topk_count = route_ids.shape[1]
    exp_here = expert_gate.shape[0]
    experts_all = exp_here * lax.axis_size("sp")
    capacity = 5 * seq_dev * topk_count // (4 * experts_all)
    score_scale = half_dim ** (-0.5)
    query_pos = lax.axis_index("sp") * seq_dev + jnp.arange(seq_dev, dtype=jnp.int32)
    query_heads = query_rows.reshape(seq_dev, heads_here, 2, half_dim)
    key_piece = lax.all_gather(key_rows, "sp", axis=0, tiled=True)
    value_piece = lax.all_gather(value_rows, "sp", axis=0, tiled=True)
    piece_len = key_piece.shape[0]
    key_heads = key_piece.reshape(piece_len, heads_here, 2, half_dim)
    value_heads = value_piece.reshape(piece_len, heads_here, head_dim)
    scores = (
        jnp.einsum("qhmd,khmd->mhqk", query_heads, key_heads, preferred_element_type=jnp.float32)
        * score_scale
    )
    key_pos = jnp.arange(piece_len, dtype=jnp.int32)
    visible = key_pos[None, :] <= query_pos[:, None]
    scores = jnp.where(visible, scores, masked_score)
    run_max = jnp.full((2, heads_here, seq_dev), masked_score, jnp.float32)
    new_max = jnp.maximum(run_max, jnp.max(scores, axis=-1))
    expo = jnp.where(visible, jnp.exp(scores - new_max[..., None]), 0.0)
    new_sum = jnp.sum(expo, axis=-1)
    product = jnp.einsum(
        "mhqk,khd->mhqd", expo.astype(jnp.bfloat16), value_heads, preferred_element_type=jnp.float32
    )
    summed = product / new_sum[..., None]
    diff_out = summed[0] - map_weight[:, None, None] * summed[1]
    head_out = rms_scale(diff_out, head_gain).astype(jnp.bfloat16)
    head_out = jnp.transpose(head_out, (1, 0, 2)).reshape(seq_dev, heads_here * head_dim)
    attn = jnp.dot(
        lax.all_gather(head_out, "tp", axis=1, tiled=True),
        out_proj,
        preferred_element_type=jnp.float32,
    )
    hidden_state = (residual_in.astype(jnp.float32) + attn).astype(jnp.bfloat16)
    full_rows = lax.all_gather(hidden_state, "tp", axis=1, tiled=True)
    normed = rms_scale(full_rows.astype(jnp.float32), norm_gain).astype(jnp.bfloat16)
    shared_gate_part = jnp.einsum(
        "rd,fd->rf", normed, shared_gate, preferred_element_type=jnp.float32
    )
    shared_up_part = jnp.einsum("rd,fd->rf", normed, shared_up, preferred_element_type=jnp.float32)
    shared_hidden = (jax.nn.silu(shared_gate_part) * shared_up_part).astype(jnp.bfloat16)
    slot_ids = block_slots(route_ids, experts_all, capacity)
    token_of = jnp.repeat(jnp.arange(seq_dev, dtype=jnp.int32), topk_count)
    slot_token = (
        jnp.full((experts_all * capacity,), seq_dev, jnp.int32)
        .at[slot_ids.reshape(-1)]
        .set(token_of)
    )
    own_cols = lax.dynamic_slice_in_dim(normed, lax.axis_index("tp") * col_dev, col_dev, 1)
    padded = jnp.concatenate([own_cols, jnp.zeros((1, col_dev), jnp.bfloat16)], axis=0)
    outgoing = jnp.take(padded, slot_token, axis=0).reshape(experts_all, capacity, col_dev)
    arrived = lax.all_to_all(outgoing, "sp", split_axis=0, concat_axis=1, tiled=True)
    arrived_rows = arrived.shape[1]
    pieces = lax.all_gather(arrived, "tp", axis=2, tiled=True)
    gate_add = jnp.einsum("erd,efd->erf", pieces, expert_gate, preferred_element_type=jnp.float32)
    up_add = jnp.einsum("erd,efd->erf", pieces, expert_up, preferred_element_type=jnp.float32)
    expert_hidden = (jax.nn.silu(gate_add) * up_add).astype(jnp.bfloat16)
    expert_flat = expert_hidden.reshape(exp_here * arrived_rows, expert_hidden.shape[2])
    pieces = (
        lax.all_gather(shared_hidden, "tp", axis=1, tiled=True),
        lax.all_gather(expert_flat, "tp", axis=1, tiled=True),
    )
    piece_width = pieces[0].shape[1]
    routed_piece = pieces[1].reshape(exp_here, arrived_rows, piece_width)
    shared_add = jnp.dot(pieces[0], shared_down, preferred_element_type=jnp.float32)
    expert_add = jnp.einsum(
        "erf,efd->erd", routed_piece, expert_down, preferred_element_type=jnp.float32
    )
    returned_rows = lax.all_to_all(
        expert_add.astype(jnp.bfloat16), "sp", split_axis=1, concat_axis=0, tiled=True
    )
    returned_flat = returned_rows.reshape(experts_all * capacity, col_dev)
    picked = (
        jnp.take(returned_flat, slot_ids.reshape(-1), axis=0)
        .reshape(seq_dev, topk_count, col_dev)
        .astype(jnp.float32)
    )
    routed = jnp.sum(picked * route_weights[:, :, None], axis=1)
    return (hidden_state.astype(jnp.float32) + shared_add + routed).astype(jnp.bfloat16)


def lane_iota(rows):
    return lax.broadcasted_iota(jnp.int32, (rows, 128), 1)


def roll_half(values):
    return pltpu.roll(values, 64, 1)


def contract_last(a, b):
    return lax.dot_general(a, b, (((1,), (1,)), ((), ())), preferred_element_type=jnp.float32)


def layer_kernel(
    n_sp,
    n_tp,
    q_in,
    k_in,
    v_in,
    res_in,
    map_w,
    head_g,
    norm_g,
    ids_in,
    route_w,
    out_proj,
    exp_gate,
    exp_up,
    exp_down,
    sh_gate,
    sh_up,
    sh_down,
    out_ref,
    w_out,
    w_gate,
    w_up,
    w_down,
    w_sgate,
    w_sup,
    w_sdown,
    kv_out,
    q_out,
    kv_buf,
    q_buf,
    o_out,
    ho_buf,
    hid_buf,
    disp_out,
    arr_buf,
    sh_buf,
    eh_buf,
    res_out,
    ret_buf,
    spread_buf,
    pick_buf,
    weight_buf,
    w_sem,
    a_send,
    kv_recv,
    q_recv,
    o_send,
    o_recv,
    d_send,
    d_recv,
    r_send,
    r_recv,
    g_send,
    g_recv,
):
    me_s = lax.axis_index("sp")
    me_t = lax.axis_index("tp")
    sib = me_t + 1 - 2 * lax.rem(me_t, 2)
    peers = n_tp // 2 - 1
    rows = res_in.shape[0]
    col_dev = res_in.shape[1]
    half = rows // 2
    quarter = rows // 4
    cap = arr_buf.shape[2]
    half_dim = 32
    groups = eh_buf.shape[1]
    per_group = n_sp // groups
    bf16 = jnp.bfloat16
    f32 = jnp.float32

    def across(k):
        other = me_s
        for b in range(n_sp.bit_length() - 1):
            if k >> b & 1:
                bit = lax.rem(me_s // (1 << b), 2)
                other = other + (1 << b) * (1 - 2 * bit)
        return other

    loads = []
    for i, (src, dst) in enumerate(
        (
            (out_proj, w_out),
            (sh_gate, w_sgate),
            (sh_up, w_sup),
            (exp_gate.at[0], w_gate),
            (exp_up.at[0], w_up),
            (exp_down.at[0], w_down),
            (sh_down, w_sdown),
        )
    ):
        copy = pltpu.make_async_copy(src, dst, w_sem.at[i])
        copy.start()
        loads.append(copy)

    barrier = pltpu.get_barrier_semaphore()
    for d in range(1, n_sp):
        pl.semaphore_signal(
            barrier, inc=1, device_id={"sp": lax.rem(me_s + d, n_sp)}, device_id_type=MESH
        )
    for d in range(1, n_tp):
        pl.semaphore_signal(
            barrier, inc=1, device_id={"tp": lax.rem(me_t + d, n_tp)}, device_id_type=MESH
        )

    sends = []

    def send(src, dst, ssem, rsem, device):
        copy = pltpu.make_async_remote_copy(
            src_ref=src,
            dst_ref=dst,
            send_sem=ssem,
            recv_sem=rsem,
            device_id=device,
            device_id_type=MESH,
        )
        copy.start()
        return copy

    def wait_recv(ref, ssem, rsem, device):
        pltpu.make_async_remote_copy(
            src_ref=ref,
            dst_ref=ref,
            send_sem=ssem,
            recv_sem=rsem,
            device_id=device,
            device_id_type=MESH,
        ).wait_recv()

    n_gs = 1 + 2 * peers

    def gather_start(piece, get):
        for k in range(1, peers + 1):
            other = lax.rem(me_t + 2 * k, n_tp)
            sends.append(
                send(
                    get(me_t),
                    get(me_t),
                    g_send.at[piece * n_gs + k],
                    g_recv.at[piece * n_tp + me_t],
                    {"tp": other},
                )
            )
        sends.append(
            send(
                get(me_t),
                get(me_t),
                g_send.at[piece * n_gs],
                g_recv.at[piece * n_tp + me_t],
                {"tp": sib},
            )
        )

    def gather_relay(piece, get):
        for k in range(1, peers + 1):
            other = lax.rem(me_t + 2 * k, n_tp)
            wait_recv(
                get(other), g_send.at[piece * n_gs], g_recv.at[piece * n_tp + other], {"tp": sib}
            )
            sends.append(
                send(
                    get(other),
                    get(other),
                    g_send.at[piece * n_gs + peers + k],
                    g_recv.at[piece * n_tp + other],
                    {"tp": sib},
                )
            )

    def gather_finish(piece, get):
        for k in range(peers + 1):
            other = lax.rem(sib + 2 * k, n_tp)
            wait_recv(
                get(other), g_send.at[piece * n_gs], g_recv.at[piece * n_tp + other], {"tp": sib}
            )

    low_rows = lane_iota(rows) < 64
    low_quarter = lane_iota(quarter) < 64
    for j in range(n_sp // 4):
        pair = slice(j * 128, (j + 1) * 128)
        keys = k_in[:, pair].astype(f32)
        vals = v_in[:, pair].astype(f32)
        kv_out[2 * j] = jnp.where(low_rows, keys, roll_half(vals)).astype(bf16)
        kv_out[2 * j + 1] = jnp.where(low_rows, roll_half(keys), vals).astype(bf16)
        for p in range(2):
            first = q_in[p * half : p * half + quarter, pair].astype(f32)
            second = q_in[p * half + quarter : (p + 1) * half, pair].astype(f32)
            q_out[4 * j + p] = jnp.where(low_quarter, first, roll_half(second)).astype(bf16)
            q_out[4 * j + 2 + p] = jnp.where(low_quarter, roll_half(first), second).astype(bf16)

    pl.semaphore_wait(barrier, n_sp + n_tp - 2)

    for d in (6, 7, 4, 5, 2, 3, 1):
        dst = across(d)
        sends.append(
            send(
                kv_out.at[dst // 2],
                kv_buf.at[me_s],
                a_send.at[2 * d],
                kv_recv.at[me_s],
                {"sp": dst},
            )
        )
        sends.append(
            send(
                q_out.at[dst], q_buf.at[me_s], a_send.at[2 * d + 1], q_recv.at[me_s], {"sp": dst}
            )
        )
    kv_buf[me_s] = kv_out[me_s // 2]
    q_buf[me_s] = q_out[me_s]

    eye = lax.broadcasted_iota(jnp.int32, (rows, rows), 0)
    eye_lane = lax.broadcasted_iota(jnp.int32, (rows, rows), 1)
    same = eye == eye_lane
    before_col = eye_lane < eye
    before_row = eye < eye_lane

    def as_column(row):
        return jnp.sum(jnp.where(same, row, 0.0), axis=1, keepdims=True)

    ids_row = [jnp.bitwise_xor(ids_in[c : c + 1, :], me_s).astype(f32) for c in range(2)]
    ids_col = [as_column(row) for row in ids_row]
    weight_col = [as_column(route_w[c : c + 1, :]) for c in range(2)]
    slot_row = []
    slot_col = []
    for c in range(2):
        hit = (ids_row[0] == ids_col[c]) | (ids_row[1] == ids_col[c])
        count = jnp.sum(jnp.where(hit & before_col, 1.0, 0.0), axis=1, keepdims=True)
        slot_col.append(ids_col[c] * cap + count)
        hit = (ids_col[0] == ids_row[c]) | (ids_col[1] == ids_row[c])
        count = jnp.sum(jnp.where(hit & before_row, 1.0, 0.0), axis=0, keepdims=True)
        slot_row.append(ids_row[c] * cap + count)
    slots = n_sp * cap
    slot_iota = lax.broadcasted_iota(jnp.int32, (slots, rows), 0).astype(f32)
    chosen = (slot_iota == slot_row[0]) | (slot_iota == slot_row[1])
    spread_buf[...] = jnp.where(chosen, 1.0, 0.0).astype(bf16)
    col_iota = lax.broadcasted_iota(jnp.int32, (rows, slots), 1).astype(f32)
    for c in range(2):
        pick_buf[c] = jnp.where(col_iota == slot_col[c], 1.0, 0.0).astype(bf16)
        weight_buf[c] = jnp.broadcast_to(weight_col[c], (rows, 128))
    head_lane = lax.broadcasted_iota(jnp.int32, map_w.shape, 1)
    map_here = jnp.sum(
        jnp.where(head_lane == me_s // 2, map_w[...], 0.0), axis=1, keepdims=True
    )
    gain_here = jnp.concatenate([jnp.zeros((1, 64), f32), head_g[...]], axis=1)

    parity = lax.rem(me_s, 2)
    lane_q = lane_iota(quarter)
    scale = half_dim ** (-0.5)
    row_in = lax.broadcasted_iota(jnp.int32, (half, rows), 0) + parity * half
    visible_half = lax.broadcasted_iota(jnp.int32, (half, rows), 1) <= row_in
    visible = jnp.concatenate([visible_half.astype(f32)] * 2, axis=0) > 0.5
    high_lanes = lane_iota(half) >= 64
    zero_q = jnp.zeros((quarter, 128), f32)
    first_map = lane_q < 32
    second_map = (lane_q >= 32) & (lane_q < 64)
    batch = n_sp // 2
    for start in range(0, n_sp, batch):
        steps = range(start, start + batch)
        for s in steps:

            @pl.when(me_s != s)
            def _():
                wait_recv(kv_buf.at[s], a_send.at[0], kv_recv.at[s], {"sp": s})
                wait_recv(q_buf.at[s], a_send.at[1], q_recv.at[s], {"sp": s})

        queries = {}
        for s in steps:
            packed = q_buf[s].astype(f32)
            rolled = roll_half(packed)
            queries[s] = jnp.concatenate(
                [
                    jnp.where(first_map, packed, zero_q),
                    jnp.where(first_map, rolled, zero_q),
                    jnp.where(second_map, packed, zero_q),
                    jnp.where(second_map, rolled, zero_q),
                ],
                axis=0,
            ).astype(bf16)
        keys = {s: kv_buf[0 : s + 1].reshape((s + 1) * rows, 128) for s in steps}
        scores = {}
        for s in steps:
            raw = contract_last(queries[s], keys[s]) * scale
            diag = jnp.where(visible, raw[:, s * rows :], masked_score)
            scores[s] = jnp.concatenate([raw[:, : s * rows], diag], axis=1) if s else diag
        row_max = {s: jnp.max(scores[s], axis=1, keepdims=True) for s in steps}
        expo = {s: jnp.exp(scores[s] - row_max[s]) for s in steps}
        total = {s: jnp.sum(expo[s], axis=1, keepdims=True) for s in steps}
        acc = {
            s: jnp.dot(expo[s].astype(bf16), keys[s], preferred_element_type=f32) for s in steps
        }
        diff = {}
        for s in steps:
            summed = acc[s] / total[s]
            raw = summed[0:half] - map_here * summed[half:rows]
            diff[s] = jnp.where(high_lanes, raw, 0.0)
        for s in steps:
            squares = jnp.sum(diff[s] * diff[s], axis=1, keepdims=True) * (1.0 / 64.0)
            head = diff[s] * lax.rsqrt(squares + epsilon) * gain_here
            o_out[s] = (roll_half(head[0:quarter]) + head[quarter:half]).astype(bf16)

        for s in steps:

            @pl.when(me_s != s)
            def _():
                send(
                    o_out.at[s],
                    ho_buf.at[me_t, me_s],
                    o_send.at[s],
                    o_recv.at[me_s],
                    {"sp": s},
                )

            @pl.when(me_s == s)
            def _():
                ho_buf[me_t, s] = o_out[s]

    split = n_sp // 2
    near = me_s // split * split

    def get_near(t):
        return ho_buf.at[t, pl.ds(near, split)]

    def get_far(t):
        return ho_buf.at[t, pl.ds(split - near, split)]

    for d in range(1, n_sp):
        if d == split:
            gather_start(0, get_near)
        other = across(d)
        wait_recv(ho_buf.at[me_t, other], o_send.at[d], o_recv.at[other], {"sp": other})
    gather_start(3 + n_sp + groups, get_far)
    for piece, get in ((0, get_near), (3 + n_sp + groups, get_far)):
        gather_relay(piece, get)
    for piece, get in ((0, get_near), (3 + n_sp + groups, get_far)):
        gather_finish(piece, get)

    blocks = []
    for p in range(2):
        for u in range(2):
            parts = []
            for t in range(n_tp):
                for j in range(n_sp // 4):
                    even = ho_buf[t, 4 * j + p].astype(f32)
                    odd = ho_buf[t, 4 * j + 2 + p].astype(f32)
                    if u == 0:
                        part = jnp.where(low_quarter, even, roll_half(odd))
                    else:
                        part = jnp.where(low_quarter, roll_half(even), odd)
                    parts.append(part.astype(bf16))
            blocks.append(jnp.concatenate(parts, axis=1))
    heads = jnp.concatenate(blocks, axis=0)
    loads[0].wait()
    attn = jnp.dot(heads, w_out[...], preferred_element_type=f32)
    hidden = (res_in[...].astype(f32) + attn).astype(bf16)
    hid_buf[me_t] = hidden

    def get_hid(t):
        return hid_buf.at[t]

    gather_start(1, get_hid)

    outgoing = jnp.dot(spread_buf[cap:slots], hidden, preferred_element_type=f32).astype(bf16)
    disp_out[1:n_sp] = outgoing.reshape(n_sp - 1, cap, col_dev)
    for d in range(1, n_sp):
        sends.append(
            send(
                disp_out.at[d],
                arr_buf.at[me_t, d],
                d_send.at[d],
                d_recv.at[d],
                {"sp": across(d)},
            )
        )

    def get_arr(d):
        return lambda t: arr_buf.at[t, d]

    def normalise(pieces):
        full = [piece.astype(f32) for piece in pieces]
        squares = sum(jnp.sum(piece * piece, axis=1, keepdims=True) for piece in full)
        factor = lax.rsqrt(squares * (1.0 / (n_tp * col_dev)) + epsilon)
        return jnp.concatenate(
            [
                (piece * factor * norm_g[:, t * col_dev : (t + 1) * col_dev]).astype(bf16)
                for t, piece in enumerate(full)
            ],
            axis=1,
        )

    def gated(normed, gate, up):
        gate_part = contract_last(normed, gate[...])
        up_part = contract_last(normed, up[...])
        return (gate_part / (1.0 + jnp.exp(-gate_part)) * up_part).astype(bf16)

    def arrive(d):
        wait_recv(arr_buf.at[me_t, d], d_send.at[d], d_recv.at[d], {"sp": across(d)})
        gather_start(2 + d, get_arr(d))

    def relay(d):
        gather_relay(2 + d, get_arr(d))

    def get_sh(t):
        return sh_buf.at[t]

    def get_eh(g):
        return lambda t: eh_buf.at[t, g]

    piece_sh = 2 + n_sp
    piece_eh = 3 + n_sp

    def expert_up(g):
        ds = range(g * per_group, (g + 1) * per_group)
        for d in ds:
            if d:
                gather_finish(2 + d, get_arr(d))
        normed = normalise(
            [
                arr_buf[t, g * per_group : (g + 1) * per_group].reshape(per_group * cap, col_dev)
                for t in range(n_tp)
            ]
        )
        eh_buf[me_t, g] = gated(normed, w_gate, w_up)

    def expert_out(g):
        gather_finish(piece_eh + g, get_eh(g))
        joined = jnp.concatenate([eh_buf[t, g] for t in range(n_tp)], axis=1)
        result = jnp.dot(joined, w_down[...], preferred_element_type=f32).astype(bf16)
        res_out[g * per_group : (g + 1) * per_group] = result.reshape(per_group, cap, col_dev)
        for d in range(g * per_group, (g + 1) * per_group):
            if d == 0:
                ret_buf[0] = res_out[0]
            else:
                sends.append(
                    send(
                        res_out.at[d],
                        ret_buf.at[d],
                        r_send.at[d],
                        r_recv.at[d],
                        {"sp": across(d)},
                    )
                )

    def relay_eh(g):
        gather_relay(piece_eh + g, get_eh(g))

    def start_eh(g):
        gather_start(piece_eh + g, get_eh(g))

    def relay_eh(g):
        gather_relay(piece_eh + g, get_eh(g))

    arrive(1)
    arrive(2)
    gather_relay(1, get_hid)
    arrive(3)
    relay(1)
    relay(2)
    arrive(4)
    gather_finish(1, get_hid)
    loads[1].wait()
    loads[2].wait()
    normed_own = normalise([hid_buf[t] for t in range(n_tp)])
    sh_buf[me_t] = gated(normed_own, w_sgate, w_sup)
    relay(3)
    arrive(5)
    relay(4)
    for t in range(n_tp):
        arr_buf[t, 0] = jnp.dot(
            spread_buf[0:cap], hid_buf[t], preferred_element_type=f32
        ).astype(bf16)
    for i in range(3, 7):
        loads[i].wait()
    expert_up(0)
    arrive(6)
    relay(5)
    expert_up(2)
    start_eh(2)
    arrive(7)
    relay(6)
    expert_up(1)
    relay_eh(2)
    relay(7)
    expert_out(2)
    expert_up(3)
    start_eh(3)
    start_eh(1)
    start_eh(0)
    gather_start(piece_sh, get_sh)
    relay_eh(3)
    expert_out(3)
    relay_eh(1)
    relay_eh(0)
    gather_relay(piece_sh, get_sh)
    expert_out(1)
    expert_out(0)

    gather_finish(piece_sh, get_sh)
    shared_all = jnp.concatenate([sh_buf[t] for t in range(n_tp)], axis=1)
    result = hid_buf[me_t].astype(f32) + jnp.dot(
        shared_all, w_sdown[...], preferred_element_type=f32
    )
    for d in range(1, n_sp):
        wait_recv(ret_buf.at[d], r_send.at[d], r_recv.at[d], {"sp": across(d)})
    returned = ret_buf[...].reshape(slots, col_dev)
    for c in range(2):
        picked = jnp.dot(pick_buf[c], returned, preferred_element_type=f32)
        result = result + weight_buf[c][:, 0:1] * picked
    out_ref[...] = result.astype(out_ref.dtype)

    for copy in sends:
        copy.wait_send()
    for s in range(n_sp):

        @pl.when(me_s != s)
        def _():
            pltpu.make_async_remote_copy(
                src_ref=o_out.at[s],
                dst_ref=ho_buf.at[me_t, me_s],
                send_sem=o_send.at[s],
                recv_sem=o_recv.at[me_s],
                device_id={"sp": s},
                device_id_type=MESH,
            ).wait_send()


def fused_body(
    residual_in,
    query_rows,
    key_rows,
    value_rows,
    map_weight,
    head_gain,
    out_proj,
    norm_gain,
    route_ids,
    route_weights,
    expert_gate,
    expert_up,
    expert_down,
    shared_gate,
    shared_up,
    shared_down,
):
    n_sp = lax.axis_size("sp")
    n_tp = lax.axis_size("tp")
    rows, col_dev = residual_in.shape
    topk = route_ids.shape[1]
    capacity = 5 * rows * topk // (4 * n_sp)
    cap = (capacity + 15) // 16 * 16
    hid_units = shared_gate.shape[0]
    bf16 = jnp.bfloat16
    groups = n_sp // 2
    pieces = 4 + n_sp + groups
    n_gs = 1 + 2 * (n_tp // 2 - 1)
    dma = pltpu.SemaphoreType.DMA
    vmem = pl.BlockSpec(memory_space=pltpu.VMEM)
    hbm = pl.BlockSpec(memory_space=pl.ANY)
    return pl.pallas_call(
        functools.partial(layer_kernel, n_sp, n_tp),
        out_shape=jax.ShapeDtypeStruct((rows, col_dev), bf16),
        in_specs=[vmem] * 9 + [hbm] * 7,
        out_specs=vmem,
        scratch_shapes=[
            pltpu.VMEM(out_proj.shape, bf16),
            pltpu.VMEM(expert_gate.shape[1:], bf16),
            pltpu.VMEM(expert_up.shape[1:], bf16),
            pltpu.VMEM(expert_down.shape[1:], bf16),
            pltpu.VMEM(shared_gate.shape, bf16),
            pltpu.VMEM(shared_up.shape, bf16),
            pltpu.VMEM(shared_down.shape, bf16),
            pltpu.VMEM((n_sp // 2, rows, 128), bf16),
            pltpu.VMEM((n_sp, rows // 4, 128), bf16),
            pltpu.VMEM((n_sp, rows, 128), bf16),
            pltpu.VMEM((n_sp, rows // 4, 128), bf16),
            pltpu.VMEM((n_sp, rows // 4, 128), bf16),
            pltpu.VMEM((n_tp, n_sp, rows // 4, 128), bf16),
            pltpu.VMEM((n_tp, rows, col_dev), bf16),
            pltpu.VMEM((n_sp, cap, col_dev), bf16),
            pltpu.VMEM((n_tp, n_sp, cap, col_dev), bf16),
            pltpu.VMEM((n_tp, rows, hid_units), bf16),
            pltpu.VMEM((n_tp, groups, n_sp // groups * cap, hid_units), bf16),
            pltpu.VMEM((n_sp, cap, col_dev), bf16),
            pltpu.VMEM((n_sp, cap, col_dev), bf16),
            pltpu.VMEM((n_sp * cap, rows), bf16),
            pltpu.VMEM((2, rows, n_sp * cap), bf16),
            pltpu.VMEM((2, rows, 128), jnp.float32),
            dma((7,)),
            dma((2 * n_sp,)),
            dma((n_sp,)),
            dma((n_sp,)),
            dma((n_sp,)),
            dma((n_sp,)),
            dma((n_sp,)),
            dma((n_sp,)),
            dma((n_sp,)),
            dma((n_sp,)),
            dma((pieces * n_gs,)),
            dma((pieces * n_tp,)),
        ],
        compiler_params=pltpu.CompilerParams(collective_id=0, has_side_effects=True),
    )(
        query_rows,
        key_rows,
        value_rows,
        residual_in,
        map_weight[None, :],
        head_gain[None, :],
        norm_gain[None, :],
        route_ids.T,
        route_weights.T,
        out_proj,
        expert_gate,
        expert_up,
        expert_down,
        shared_gate,
        shared_up,
        shared_down,
    )


def layer(*args):
    residual_in, map_weight, head_gain, route_ids = args[0], args[4], args[5], args[8]
    fits = (
        2 * map_weight.shape[0] == lax.axis_size("sp") == 8
        and map_weight.shape[0] % 2 == 0
        and head_gain.shape[0] == 64
        and route_ids.shape[1] == 2
        and args[10].shape[0] == 1
        and residual_in.shape[0] % 64 == 0
        and residual_in.shape[1] % 128 == 0
        and args[13].shape[0] % 128 == 0
        and lax.axis_size("tp") % 2 == 0
    )
    return (fused_body if fits else body)(*args)


def solution(mesh):
    in_specs = (
        P("sp", "tp"),
        P("sp", "tp"),
        P("sp", "tp"),
        P("sp", "tp"),
        P("tp"),
        P(),
        P(None, "tp"),
        P(),
        P("sp", None),
        P("sp", None),
        P("sp", "tp", None),
        P("sp", "tp", None),
        P("sp", None, "tp"),
        P("tp", None),
        P("tp", None),
        P(None, "tp"),
    )
    out_specs = P("sp", "tp")
    return jax.shard_map(layer, mesh=mesh, in_specs=in_specs, out_specs=out_specs, check_vma=False)
```

```python
import functools

import jax
import jax.numpy as jnp
from jax import lax
from jax.experimental import pallas as pl
from jax.experimental.pallas import tpu as pltpu
from jax.sharding import PartitionSpec as P

epsilon = 1e-06
masked_score = -1e30
MESH = pl.DeviceIdType.MESH


def rms_scale(values, gain_vec):
    squares = jnp.mean(values * values, axis=-1, keepdims=True)
    return values * lax.rsqrt(squares + epsilon) * gain_vec


def block_slots(route_block, experts_all, capacity):
    flat_ids = route_block.reshape(-1)
    one_hot = (flat_ids[:, None] == jnp.arange(experts_all, dtype=jnp.int32)[None, :]).astype(
        jnp.int32
    )
    earlier = jnp.cumsum(one_hot, axis=0) - one_hot
    position = jnp.sum(earlier * one_hot, axis=1)
    return (flat_ids * capacity + position).reshape(route_block.shape)


def body(
    residual_in,
    query_rows,
    key_rows,
    value_rows,
    map_weight,
    head_gain,
    out_proj,
    norm_gain,
    route_ids,
    route_weights,
    expert_gate,
    expert_up,
    expert_down,
    shared_gate,
    shared_up,
    shared_down,
):
    seq_dev = residual_in.shape[0]
    col_dev = residual_in.shape[1]
    heads_here = map_weight.shape[0]
    head_dim = head_gain.shape[0]
    half_dim = head_dim // 2
    topk_count = route_ids.shape[1]
    exp_here = expert_gate.shape[0]
    experts_all = exp_here * lax.axis_size("sp")
    capacity = 5 * seq_dev * topk_count // (4 * experts_all)
    score_scale = half_dim ** (-0.5)
    query_pos = lax.axis_index("sp") * seq_dev + jnp.arange(seq_dev, dtype=jnp.int32)
    query_heads = query_rows.reshape(seq_dev, heads_here, 2, half_dim)
    key_piece = lax.all_gather(key_rows, "sp", axis=0, tiled=True)
    value_piece = lax.all_gather(value_rows, "sp", axis=0, tiled=True)
    piece_len = key_piece.shape[0]
    key_heads = key_piece.reshape(piece_len, heads_here, 2, half_dim)
    value_heads = value_piece.reshape(piece_len, heads_here, head_dim)
    scores = (
        jnp.einsum("qhmd,khmd->mhqk", query_heads, key_heads, preferred_element_type=jnp.float32)
        * score_scale
    )
    key_pos = jnp.arange(piece_len, dtype=jnp.int32)
    visible = key_pos[None, :] <= query_pos[:, None]
    scores = jnp.where(visible, scores, masked_score)
    run_max = jnp.full((2, heads_here, seq_dev), masked_score, jnp.float32)
    new_max = jnp.maximum(run_max, jnp.max(scores, axis=-1))
    expo = jnp.where(visible, jnp.exp(scores - new_max[..., None]), 0.0)
    new_sum = jnp.sum(expo, axis=-1)
    product = jnp.einsum(
        "mhqk,khd->mhqd", expo.astype(jnp.bfloat16), value_heads, preferred_element_type=jnp.float32
    )
    summed = product / new_sum[..., None]
    diff_out = summed[0] - map_weight[:, None, None] * summed[1]
    head_out = rms_scale(diff_out, head_gain).astype(jnp.bfloat16)
    head_out = jnp.transpose(head_out, (1, 0, 2)).reshape(seq_dev, heads_here * head_dim)
    attn = jnp.dot(
        lax.all_gather(head_out, "tp", axis=1, tiled=True),
        out_proj,
        preferred_element_type=jnp.float32,
    )
    hidden_state = (residual_in.astype(jnp.float32) + attn).astype(jnp.bfloat16)
    full_rows = lax.all_gather(hidden_state, "tp", axis=1, tiled=True)
    normed = rms_scale(full_rows.astype(jnp.float32), norm_gain).astype(jnp.bfloat16)
    shared_gate_part = jnp.einsum(
        "rd,fd->rf", normed, shared_gate, preferred_element_type=jnp.float32
    )
    shared_up_part = jnp.einsum("rd,fd->rf", normed, shared_up, preferred_element_type=jnp.float32)
    shared_hidden = (jax.nn.silu(shared_gate_part) * shared_up_part).astype(jnp.bfloat16)
    slot_ids = block_slots(route_ids, experts_all, capacity)
    token_of = jnp.repeat(jnp.arange(seq_dev, dtype=jnp.int32), topk_count)
    slot_token = (
        jnp.full((experts_all * capacity,), seq_dev, jnp.int32)
        .at[slot_ids.reshape(-1)]
        .set(token_of)
    )
    own_cols = lax.dynamic_slice_in_dim(normed, lax.axis_index("tp") * col_dev, col_dev, 1)
    padded = jnp.concatenate([own_cols, jnp.zeros((1, col_dev), jnp.bfloat16)], axis=0)
    outgoing = jnp.take(padded, slot_token, axis=0).reshape(experts_all, capacity, col_dev)
    arrived = lax.all_to_all(outgoing, "sp", split_axis=0, concat_axis=1, tiled=True)
    arrived_rows = arrived.shape[1]
    pieces = lax.all_gather(arrived, "tp", axis=2, tiled=True)
    gate_add = jnp.einsum("erd,efd->erf", pieces, expert_gate, preferred_element_type=jnp.float32)
    up_add = jnp.einsum("erd,efd->erf", pieces, expert_up, preferred_element_type=jnp.float32)
    expert_hidden = (jax.nn.silu(gate_add) * up_add).astype(jnp.bfloat16)
    expert_flat = expert_hidden.reshape(exp_here * arrived_rows, expert_hidden.shape[2])
    pieces = (
        lax.all_gather(shared_hidden, "tp", axis=1, tiled=True),
        lax.all_gather(expert_flat, "tp", axis=1, tiled=True),
    )
    piece_width = pieces[0].shape[1]
    routed_piece = pieces[1].reshape(exp_here, arrived_rows, piece_width)
    shared_add = jnp.dot(pieces[0], shared_down, preferred_element_type=jnp.float32)
    expert_add = jnp.einsum(
        "erf,efd->erd", routed_piece, expert_down, preferred_element_type=jnp.float32
    )
    returned_rows = lax.all_to_all(
        expert_add.astype(jnp.bfloat16), "sp", split_axis=1, concat_axis=0, tiled=True
    )
    returned_flat = returned_rows.reshape(experts_all * capacity, col_dev)
    picked = (
        jnp.take(returned_flat, slot_ids.reshape(-1), axis=0)
        .reshape(seq_dev, topk_count, col_dev)
        .astype(jnp.float32)
    )
    routed = jnp.sum(picked * route_weights[:, :, None], axis=1)
    return (hidden_state.astype(jnp.float32) + shared_add + routed).astype(jnp.bfloat16)


def lane_iota(rows):
    return lax.broadcasted_iota(jnp.int32, (rows, 128), 1)


def roll_half(values):
    return pltpu.roll(values, 64, 1)


def contract_last(a, b):
    return lax.dot_general(a, b, (((1,), (1,)), ((), ())), preferred_element_type=jnp.float32)


def layer_kernel(
    n_sp,
    n_tp,
    q_in,
    k_in,
    v_in,
    res_in,
    map_w,
    head_g,
    norm_g,
    ids_in,
    route_w,
    out_proj,
    exp_gate,
    exp_up,
    exp_down,
    sh_gate,
    sh_up,
    sh_down,
    out_ref,
    w_out,
    w_gate,
    w_up,
    w_down,
    w_sgate,
    w_sup,
    w_sdown,
    kv_out,
    q_out,
    kv_buf,
    q_buf,
    o_out,
    ho_buf,
    hid_buf,
    disp_out,
    arr_buf,
    sh_buf,
    eh_buf,
    res_out,
    ret_buf,
    spread_buf,
    pick_buf,
    weight_buf,
    w_sem,
    a_send,
    kv_recv,
    q_recv,
    o_send,
    o_recv,
    d_send,
    d_recv,
    r_send,
    r_recv,
    g_send,
    g_recv,
):
    me_s = lax.axis_index("sp")
    me_t = lax.axis_index("tp")
    sib = me_t + 1 - 2 * lax.rem(me_t, 2)
    peers = n_tp // 2 - 1
    rows = res_in.shape[0]
    col_dev = res_in.shape[1]
    half = rows // 2
    quarter = rows // 4
    cap = arr_buf.shape[2]
    half_dim = 32
    groups = eh_buf.shape[1]
    per_group = n_sp // groups
    bf16 = jnp.bfloat16
    f32 = jnp.float32

    def across(k):
        other = me_s
        for b in range(n_sp.bit_length() - 1):
            if k >> b & 1:
                bit = lax.rem(me_s // (1 << b), 2)
                other = other + (1 << b) * (1 - 2 * bit)
        return other

    loads = []
    for i, (src, dst) in enumerate(
        (
            (out_proj, w_out),
            (sh_gate, w_sgate),
            (sh_up, w_sup),
            (exp_gate.at[0], w_gate),
            (exp_up.at[0], w_up),
            (exp_down.at[0], w_down),
            (sh_down, w_sdown),
        )
    ):
        copy = pltpu.make_async_copy(src, dst, w_sem.at[i])
        copy.start()
        loads.append(copy)

    barrier = pltpu.get_barrier_semaphore()
    for d in range(1, n_sp):
        pl.semaphore_signal(
            barrier, inc=1, device_id={"sp": lax.rem(me_s + d, n_sp)}, device_id_type=MESH
        )
    for d in range(1, n_tp):
        pl.semaphore_signal(
            barrier, inc=1, device_id={"tp": lax.rem(me_t + d, n_tp)}, device_id_type=MESH
        )

    sends = []

    def send(src, dst, ssem, rsem, device):
        copy = pltpu.make_async_remote_copy(
            src_ref=src,
            dst_ref=dst,
            send_sem=ssem,
            recv_sem=rsem,
            device_id=device,
            device_id_type=MESH,
        )
        copy.start()
        return copy

    def wait_recv(ref, ssem, rsem, device):
        pltpu.make_async_remote_copy(
            src_ref=ref,
            dst_ref=ref,
            send_sem=ssem,
            recv_sem=rsem,
            device_id=device,
            device_id_type=MESH,
        ).wait_recv()

    n_gs = 1 + 2 * peers

    def gather_start(piece, get):
        for k in range(1, peers + 1):
            other = lax.rem(me_t + 2 * k, n_tp)
            sends.append(
                send(
                    get(me_t),
                    get(me_t),
                    g_send.at[piece * n_gs + k],
                    g_recv.at[piece * n_tp + me_t],
                    {"tp": other},
                )
            )
        sends.append(
            send(
                get(me_t),
                get(me_t),
                g_send.at[piece * n_gs],
                g_recv.at[piece * n_tp + me_t],
                {"tp": sib},
            )
        )

    def gather_relay(piece, get):
        for k in range(1, peers + 1):
            other = lax.rem(me_t + 2 * k, n_tp)
            wait_recv(
                get(other), g_send.at[piece * n_gs], g_recv.at[piece * n_tp + other], {"tp": sib}
            )
            sends.append(
                send(
                    get(other),
                    get(other),
                    g_send.at[piece * n_gs + peers + k],
                    g_recv.at[piece * n_tp + other],
                    {"tp": sib},
                )
            )

    def gather_finish(piece, get):
        for k in range(peers + 1):
            other = lax.rem(sib + 2 * k, n_tp)
            wait_recv(
                get(other), g_send.at[piece * n_gs], g_recv.at[piece * n_tp + other], {"tp": sib}
            )

    low_rows = lane_iota(rows) < 64
    low_quarter = lane_iota(quarter) < 64
    for j in range(n_sp // 4):
        pair = slice(j * 128, (j + 1) * 128)
        keys = k_in[:, pair].astype(f32)
        vals = v_in[:, pair].astype(f32)
        kv_out[2 * j] = jnp.where(low_rows, keys, roll_half(vals)).astype(bf16)
        kv_out[2 * j + 1] = jnp.where(low_rows, roll_half(keys), vals).astype(bf16)
        for p in range(2):
            first = q_in[p * half : p * half + quarter, pair].astype(f32)
            second = q_in[p * half + quarter : (p + 1) * half, pair].astype(f32)
            q_out[4 * j + p] = jnp.where(low_quarter, first, roll_half(second)).astype(bf16)
            q_out[4 * j + 2 + p] = jnp.where(low_quarter, roll_half(first), second).astype(bf16)

    pl.semaphore_wait(barrier, n_sp + n_tp - 2)

    for d in (6, 7, 4, 5, 2, 3, 1):
        dst = across(d)
        sends.append(
            send(
                kv_out.at[dst // 2],
                kv_buf.at[me_s],
                a_send.at[2 * d],
                kv_recv.at[me_s],
                {"sp": dst},
            )
        )
        sends.append(
            send(
                q_out.at[dst], q_buf.at[me_s], a_send.at[2 * d + 1], q_recv.at[me_s], {"sp": dst}
            )
        )
    kv_buf[me_s] = kv_out[me_s // 2]
    q_buf[me_s] = q_out[me_s]

    eye = lax.broadcasted_iota(jnp.int32, (rows, rows), 0)
    eye_lane = lax.broadcasted_iota(jnp.int32, (rows, rows), 1)
    same = eye == eye_lane
    before_col = eye_lane < eye
    before_row = eye < eye_lane

    def as_column(row):
        return jnp.sum(jnp.where(same, row, 0.0), axis=1, keepdims=True)

    ids_row = [jnp.bitwise_xor(ids_in[c : c + 1, :], me_s).astype(f32) for c in range(2)]
    ids_col = [as_column(row) for row in ids_row]
    weight_col = [as_column(route_w[c : c + 1, :]) for c in range(2)]
    slot_row = []
    slot_col = []
    for c in range(2):
        hit = (ids_row[0] == ids_col[c]) | (ids_row[1] == ids_col[c])
        count = jnp.sum(jnp.where(hit & before_col, 1.0, 0.0), axis=1, keepdims=True)
        slot_col.append(ids_col[c] * cap + count)
        hit = (ids_col[0] == ids_row[c]) | (ids_col[1] == ids_row[c])
        count = jnp.sum(jnp.where(hit & before_row, 1.0, 0.0), axis=0, keepdims=True)
        slot_row.append(ids_row[c] * cap + count)
    slots = n_sp * cap
    slot_iota = lax.broadcasted_iota(jnp.int32, (slots, rows), 0).astype(f32)
    chosen = (slot_iota == slot_row[0]) | (slot_iota == slot_row[1])
    spread_buf[...] = jnp.where(chosen, 1.0, 0.0).astype(bf16)
    col_iota = lax.broadcasted_iota(jnp.int32, (rows, slots), 1).astype(f32)
    for c in range(2):
        pick_buf[c] = jnp.where(col_iota == slot_col[c], 1.0, 0.0).astype(bf16)
        weight_buf[c] = jnp.broadcast_to(weight_col[c], (rows, 128))
    head_lane = lax.broadcasted_iota(jnp.int32, map_w.shape, 1)
    map_here = jnp.sum(
        jnp.where(head_lane == me_s // 2, map_w[...], 0.0), axis=1, keepdims=True
    )
    gain_here = jnp.concatenate([jnp.zeros((1, 64), f32), head_g[...]], axis=1)

    parity = lax.rem(me_s, 2)
    lane_q = lane_iota(quarter)
    scale = half_dim ** (-0.5)
    row_in = lax.broadcasted_iota(jnp.int32, (half, rows), 0) + parity * half
    visible_half = lax.broadcasted_iota(jnp.int32, (half, rows), 1) <= row_in
    visible = jnp.concatenate([visible_half.astype(f32)] * 2, axis=0) > 0.5
    high_lanes = lane_iota(half) >= 64
    zero_q = jnp.zeros((quarter, 128), f32)
    first_map = lane_q < 32
    second_map = (lane_q >= 32) & (lane_q < 64)
    batch = n_sp // 2
    for start in range(0, n_sp, batch):
        steps = range(start, start + batch)
        for s in steps:

            @pl.when(me_s != s)
            def _():
                wait_recv(kv_buf.at[s], a_send.at[0], kv_recv.at[s], {"sp": s})
                wait_recv(q_buf.at[s], a_send.at[1], q_recv.at[s], {"sp": s})

        queries = {}
        for s in steps:
            packed = q_buf[s].astype(f32)
            rolled = roll_half(packed)
            queries[s] = jnp.concatenate(
                [
                    jnp.where(first_map, packed, zero_q),
                    jnp.where(first_map, rolled, zero_q),
                    jnp.where(second_map, packed, zero_q),
                    jnp.where(second_map, rolled, zero_q),
                ],
                axis=0,
            ).astype(bf16)
        keys = {s: kv_buf[0 : s + 1].reshape((s + 1) * rows, 128) for s in steps}
        scores = {}
        for s in steps:
            raw = contract_last(queries[s], keys[s]) * scale
            diag = jnp.where(visible, raw[:, s * rows :], masked_score)
            scores[s] = jnp.concatenate([raw[:, : s * rows], diag], axis=1) if s else diag
        row_max = {s: jnp.max(scores[s], axis=1, keepdims=True) for s in steps}
        expo = {s: jnp.exp(scores[s] - row_max[s]) for s in steps}
        total = {s: jnp.sum(expo[s], axis=1, keepdims=True) for s in steps}
        acc = {
            s: jnp.dot(expo[s].astype(bf16), keys[s], preferred_element_type=f32) for s in steps
        }
        diff = {}
        for s in steps:
            summed = acc[s] / total[s]
            raw = summed[0:half] - map_here * summed[half:rows]
            diff[s] = jnp.where(high_lanes, raw, 0.0)
        for s in steps:
            squares = jnp.sum(diff[s] * diff[s], axis=1, keepdims=True) * (1.0 / 64.0)
            head = diff[s] * lax.rsqrt(squares + epsilon) * gain_here
            o_out[s] = (roll_half(head[0:quarter]) + head[quarter:half]).astype(bf16)

        for s in steps:

            @pl.when(me_s != s)
            def _():
                send(
                    o_out.at[s],
                    ho_buf.at[me_t, me_s],
                    o_send.at[s],
                    o_recv.at[me_s],
                    {"sp": s},
                )

            @pl.when(me_s == s)
            def _():
                ho_buf[me_t, s] = o_out[s]

    split = n_sp // 2
    near = me_s // split * split

    def get_near(t):
        return ho_buf.at[t, pl.ds(near, split)]

    def get_far(t):
        return ho_buf.at[t, pl.ds(split - near, split)]

    for d in range(1, n_sp):
        if d == split:
            gather_start(0, get_near)
        other = across(d)
        wait_recv(ho_buf.at[me_t, other], o_send.at[d], o_recv.at[other], {"sp": other})
    gather_start(3 + n_sp + groups, get_far)
    for piece, get in ((0, get_near), (3 + n_sp + groups, get_far)):
        gather_relay(piece, get)
    for piece, get in ((0, get_near), (3 + n_sp + groups, get_far)):
        gather_finish(piece, get)

    blocks = []
    for p in range(2):
        for u in range(2):
            parts = []
            for t in range(n_tp):
                for j in range(n_sp // 4):
                    even = ho_buf[t, 4 * j + p].astype(f32)
                    odd = ho_buf[t, 4 * j + 2 + p].astype(f32)
                    if u == 0:
                        part = jnp.where(low_quarter, even, roll_half(odd))
                    else:
                        part = jnp.where(low_quarter, roll_half(even), odd)
                    parts.append(part.astype(bf16))
            blocks.append(jnp.concatenate(parts, axis=1))
    heads = jnp.concatenate(blocks, axis=0)
    loads[0].wait()
    attn = jnp.dot(heads, w_out[...], preferred_element_type=f32)
    hidden = (res_in[...].astype(f32) + attn).astype(bf16)
    hid_buf[me_t] = hidden

    def get_hid(t):
        return hid_buf.at[t]

    gather_start(1, get_hid)

    outgoing = jnp.dot(spread_buf[cap:slots], hidden, preferred_element_type=f32).astype(bf16)
    disp_out[1:n_sp] = outgoing.reshape(n_sp - 1, cap, col_dev)
    for d in range(1, n_sp):
        sends.append(
            send(
                disp_out.at[d],
                arr_buf.at[me_t, d],
                d_send.at[d],
                d_recv.at[d],
                {"sp": across(d)},
            )
        )

    def get_arr(d):
        return lambda t: arr_buf.at[t, d]

    def normalise(pieces):
        full = [piece.astype(f32) for piece in pieces]
        squares = sum(jnp.sum(piece * piece, axis=1, keepdims=True) for piece in full)
        factor = lax.rsqrt(squares * (1.0 / (n_tp * col_dev)) + epsilon)
        return jnp.concatenate(
            [
                (piece * factor * norm_g[:, t * col_dev : (t + 1) * col_dev]).astype(bf16)
                for t, piece in enumerate(full)
            ],
            axis=1,
        )

    def gated(normed, gate, up):
        gate_part = contract_last(normed, gate[...])
        up_part = contract_last(normed, up[...])
        return (gate_part / (1.0 + jnp.exp(-gate_part)) * up_part).astype(bf16)

    def arrive(d):
        wait_recv(arr_buf.at[me_t, d], d_send.at[d], d_recv.at[d], {"sp": across(d)})
        gather_start(2 + d, get_arr(d))

    def relay(d):
        gather_relay(2 + d, get_arr(d))

    def get_sh(t):
        return sh_buf.at[t]

    def get_eh(g):
        return lambda t: eh_buf.at[t, g]

    piece_sh = 2 + n_sp
    piece_eh = 3 + n_sp

    def expert_up(g):
        ds = range(g * per_group, (g + 1) * per_group)
        for d in ds:
            if d:
                gather_finish(2 + d, get_arr(d))
        normed = normalise(
            [
                arr_buf[t, g * per_group : (g + 1) * per_group].reshape(per_group * cap, col_dev)
                for t in range(n_tp)
            ]
        )
        eh_buf[me_t, g] = gated(normed, w_gate, w_up)

    def expert_out(g):
        gather_finish(piece_eh + g, get_eh(g))
        joined = jnp.concatenate([eh_buf[t, g] for t in range(n_tp)], axis=1)
        result = jnp.dot(joined, w_down[...], preferred_element_type=f32).astype(bf16)
        res_out[g * per_group : (g + 1) * per_group] = result.reshape(per_group, cap, col_dev)
        for d in range(g * per_group, (g + 1) * per_group):
            if d == 0:
                ret_buf[0] = res_out[0]
            else:
                sends.append(
                    send(
                        res_out.at[d],
                        ret_buf.at[d],
                        r_send.at[d],
                        r_recv.at[d],
                        {"sp": across(d)},
                    )
                )

    def relay_eh(g):
        gather_relay(piece_eh + g, get_eh(g))

    def start_eh(g):
        gather_start(piece_eh + g, get_eh(g))

    def relay_eh(g):
        gather_relay(piece_eh + g, get_eh(g))

    arrive(1)
    arrive(2)
    gather_relay(1, get_hid)
    arrive(3)
    relay(1)
    relay(2)
    arrive(4)
    gather_finish(1, get_hid)
    loads[1].wait()
    loads[2].wait()
    normed_own = normalise([hid_buf[t] for t in range(n_tp)])
    sh_buf[me_t] = gated(normed_own, w_sgate, w_sup)
    relay(3)
    arrive(5)
    relay(4)
    for t in range(n_tp):
        arr_buf[t, 0] = jnp.dot(
            spread_buf[0:cap], hid_buf[t], preferred_element_type=f32
        ).astype(bf16)
    for i in range(3, 7):
        loads[i].wait()
    expert_up(0)
    arrive(6)
    relay(5)
    expert_up(2)
    start_eh(2)
    expert_up(1)
    arrive(7)
    start_eh(1)
    start_eh(0)
    relay(6)
    relay_eh(2)
    relay(7)
    expert_out(2)
    expert_up(3)
    start_eh(3)
    gather_start(piece_sh, get_sh)
    relay_eh(1)
    relay_eh(0)
    expert_out(1)
    expert_out(0)
    relay_eh(3)
    expert_out(3)
    gather_relay(piece_sh, get_sh)

    gather_finish(piece_sh, get_sh)
    shared_all = jnp.concatenate([sh_buf[t] for t in range(n_tp)], axis=1)
    result = hid_buf[me_t].astype(f32) + jnp.dot(
        shared_all, w_sdown[...], preferred_element_type=f32
    )
    for d in range(1, n_sp):
        wait_recv(ret_buf.at[d], r_send.at[d], r_recv.at[d], {"sp": across(d)})
    returned = ret_buf[...].reshape(slots, col_dev)
    for c in range(2):
        picked = jnp.dot(pick_buf[c], returned, preferred_element_type=f32)
        result = result + weight_buf[c][:, 0:1] * picked
    out_ref[...] = result.astype(out_ref.dtype)

    for copy in sends:
        copy.wait_send()
    for s in range(n_sp):

        @pl.when(me_s != s)
        def _():
            pltpu.make_async_remote_copy(
                src_ref=o_out.at[s],
                dst_ref=ho_buf.at[me_t, me_s],
                send_sem=o_send.at[s],
                recv_sem=o_recv.at[me_s],
                device_id={"sp": s},
                device_id_type=MESH,
            ).wait_send()


def fused_body(
    residual_in,
    query_rows,
    key_rows,
    value_rows,
    map_weight,
    head_gain,
    out_proj,
    norm_gain,
    route_ids,
    route_weights,
    expert_gate,
    expert_up,
    expert_down,
    shared_gate,
    shared_up,
    shared_down,
):
    n_sp = lax.axis_size("sp")
    n_tp = lax.axis_size("tp")
    rows, col_dev = residual_in.shape
    topk = route_ids.shape[1]
    capacity = 5 * rows * topk // (4 * n_sp)
    cap = (capacity + 15) // 16 * 16
    hid_units = shared_gate.shape[0]
    bf16 = jnp.bfloat16
    groups = n_sp // 2
    pieces = 4 + n_sp + groups
    n_gs = 1 + 2 * (n_tp // 2 - 1)
    dma = pltpu.SemaphoreType.DMA
    vmem = pl.BlockSpec(memory_space=pltpu.VMEM)
    hbm = pl.BlockSpec(memory_space=pl.ANY)
    return pl.pallas_call(
        functools.partial(layer_kernel, n_sp, n_tp),
        out_shape=jax.ShapeDtypeStruct((rows, col_dev), bf16),
        in_specs=[vmem] * 9 + [hbm] * 7,
        out_specs=vmem,
        scratch_shapes=[
            pltpu.VMEM(out_proj.shape, bf16),
            pltpu.VMEM(expert_gate.shape[1:], bf16),
            pltpu.VMEM(expert_up.shape[1:], bf16),
            pltpu.VMEM(expert_down.shape[1:], bf16),
            pltpu.VMEM(shared_gate.shape, bf16),
            pltpu.VMEM(shared_up.shape, bf16),
            pltpu.VMEM(shared_down.shape, bf16),
            pltpu.VMEM((n_sp // 2, rows, 128), bf16),
            pltpu.VMEM((n_sp, rows // 4, 128), bf16),
            pltpu.VMEM((n_sp, rows, 128), bf16),
            pltpu.VMEM((n_sp, rows // 4, 128), bf16),
            pltpu.VMEM((n_sp, rows // 4, 128), bf16),
            pltpu.VMEM((n_tp, n_sp, rows // 4, 128), bf16),
            pltpu.VMEM((n_tp, rows, col_dev), bf16),
            pltpu.VMEM((n_sp, cap, col_dev), bf16),
            pltpu.VMEM((n_tp, n_sp, cap, col_dev), bf16),
            pltpu.VMEM((n_tp, rows, hid_units), bf16),
            pltpu.VMEM((n_tp, groups, n_sp // groups * cap, hid_units), bf16),
            pltpu.VMEM((n_sp, cap, col_dev), bf16),
            pltpu.VMEM((n_sp, cap, col_dev), bf16),
            pltpu.VMEM((n_sp * cap, rows), bf16),
            pltpu.VMEM((2, rows, n_sp * cap), bf16),
            pltpu.VMEM((2, rows, 128), jnp.float32),
            dma((7,)),
            dma((2 * n_sp,)),
            dma((n_sp,)),
            dma((n_sp,)),
            dma((n_sp,)),
            dma((n_sp,)),
            dma((n_sp,)),
            dma((n_sp,)),
            dma((n_sp,)),
            dma((n_sp,)),
            dma((pieces * n_gs,)),
            dma((pieces * n_tp,)),
        ],
        compiler_params=pltpu.CompilerParams(collective_id=0, has_side_effects=True),
    )(
        query_rows,
        key_rows,
        value_rows,
        residual_in,
        map_weight[None, :],
        head_gain[None, :],
        norm_gain[None, :],
        route_ids.T,
        route_weights.T,
        out_proj,
        expert_gate,
        expert_up,
        expert_down,
        shared_gate,
        shared_up,
        shared_down,
    )


def layer(*args):
    residual_in, map_weight, head_gain, route_ids = args[0], args[4], args[5], args[8]
    fits = (
        2 * map_weight.shape[0] == lax.axis_size("sp") == 8
        and map_weight.shape[0] % 2 == 0
        and head_gain.shape[0] == 64
        and route_ids.shape[1] == 2
        and args[10].shape[0] == 1
        and residual_in.shape[0] % 64 == 0
        and residual_in.shape[1] % 128 == 0
        and args[13].shape[0] % 128 == 0
        and lax.axis_size("tp") % 2 == 0
    )
    return (fused_body if fits else body)(*args)


def solution(mesh):
    in_specs = (
        P("sp", "tp"),
        P("sp", "tp"),
        P("sp", "tp"),
        P("sp", "tp"),
        P("tp"),
        P(),
        P(None, "tp"),
        P(),
        P("sp", None),
        P("sp", None),
        P("sp", "tp", None),
        P("sp", "tp", None),
        P("sp", None, "tp"),
        P("tp", None),
        P("tp", None),
        P(None, "tp"),
    )
    out_specs = P("sp", "tp")
    return jax.shard_map(layer, mesh=mesh, in_specs=in_specs, out_specs=out_specs, check_vma=False)
```
